256 devices in a mesh: grp: 2 (over y), st: 32 (over z, core), tp: 4 (over x).
Axes of the slice: x: 4, y: 2, z: 16, core: 2. Of those that a mesh axis runs over, the one named last changes fastest.
The devices are a block of a 4x16x16 slice.
Arguments:
- tokens: bfloat16 [65536, 2048], P(('grp', 'st'), 'tp'), parts along dimension 0, may hold values from -6 to 6
- norm_gain: float32 [2048], replicated, may hold values from 0.1 to 1.9
- pool_weight: bfloat16 [4, 512, 512], P('tp'), may hold values from -0.25 to 0.25
- pool_scale: float32 [2048], P('tp'), may hold values from 0.1 to 1.9
- query_weight: bfloat16 [2048, 1024], P(None, 'tp'), may hold values from -3 to 3
- gate_weight: bfloat16 [2048, 8], replicated, may hold values from -0.125 to 0.125
- key_weight: bfloat16 [2048, 1024], P(None, 'tp'), may hold values from -0.125 to 0.125
- value_weight: bfloat16 [2048, 1024], P(None, 'tp'), may hold values from -0.125 to 0.125
- out_weight: bfloat16 [1024, 2048], P(None, 'tp'), may hold values from -0.1875 to 0.1875
- passage_gain: float32 [2048], replicated, may hold values from 0.1 to 1.9
- passage_store: bfloat16 [1536, 64, 2048], P(('grp', 'st')), parts along dimension 0, may hold values from -6 to 6
- passage_ids: int32 [512, 4], P(('grp', 'st')), parts along dimension 0, may hold values from 0 to 767, as said below
Outputs:
- mixed: bfloat16 [65536, 2048], P(('grp', 'st'), 'tp'), parts along dimension 0
The draws below stay inside these ranges and needn't reach their ends.
There are 2 independent parts, one for each index of `grp`. The reference program is written for one: setup_inputs(seed, part) draws one part's arguments, and reference() takes and returns one part's arrays. A program takes and returns all parts, laid end to end along the dimension named above; an argument that names none is the same for every part. Nothing has to cross between parts.
Inputs may be any that keep to these rules, and one draw needn't show every extreme that they name: `passage_ids`: the ids of the blocks of one index of st name at most 2 passages held by any one index of st, and exactly 2 held by some index.
All inputs are finite; a program needn't handle non-finite values.
Results may differ from the reference program's by a relative error of at most 0.009.
Values may be sent and summed in bfloat16 or wider, within the bound.
No kernel may reach another device: no remote copies, remote signals or barrier semaphores. Data moves between devices by JAX's collectives and lax.ppermute only.
A program may use at most 128 MiB of HBM per device.

```python
import jax
import jax.numpy as jnp
from jax import lax

D = 2048
HEADS = 8
HD = 128
GROUPS = 4
GROUP_CH = 512
SEQ_LEN = 256
BLK = 128
NPB = 4
PLEN = 64
P_DEV = 24
TOKENS = 32768
BLK_DEV = 8
BLOCKS = 256
REQ = 32
CAP = 2
PASSAGES = 768
N_ST = 32


def draw_passage_ids(key, part):
    base_key = jax.random.fold_in(key, 11)
    slots_all = N_ST * CAP
    tickets = jnp.arange(slots_all, dtype=jnp.int32)
    ticket_owner = tickets // CAP

    def one_reader(reader_key, reader):
        order_key, full_key, shuffle_key, first_key, second_key = jax.random.split(reader_key, 5)
        base_rank = jax.random.permutation(order_key, slots_all).astype(jnp.int32)
        full_owner = jax.random.randint(full_key, (), 0, N_ST, dtype=jnp.int32)
        before = (reader + N_ST - 1) % N_ST
        halfway = (reader + N_ST // 2) % N_ST
        forced = (tickets == before * CAP) | (tickets == halfway * CAP)
        ranking = base_rank - 3 * slots_all * (ticket_owner == full_owner).astype(jnp.int32) - slots_all * forced.astype(jnp.int32)
        chosen = jnp.argsort(ranking, stable=True)[:REQ]
        owners = ticket_owner[chosen]
        owners = owners[jax.random.permutation(shuffle_key, REQ)]
        local_index = jnp.minimum(jax.random.randint(first_key, (REQ,), 0, P_DEV, dtype=jnp.int32), jax.random.randint(second_key, (REQ,), 0, P_DEV, dtype=jnp.int32))
        return (owners * P_DEV + local_index).reshape(BLK_DEV, NPB)
    reader_keys = jax.random.split(base_key, N_ST)
    readers = jnp.arange(N_ST, dtype=jnp.int32)
    return jax.vmap(one_reader)(reader_keys, readers).reshape(BLOCKS, NPB).astype(jnp.int32)


def draw_query_weight(key, part):
    base_key = jax.random.fold_in(key, 23)
    normal_key = jax.random.fold_in(base_key, 0)
    weights = jax.random.normal(normal_key, (D, HEADS * HD), jnp.float32) * D ** (-0.5)
    return jnp.clip(weights, -3.0, 3.0).astype(jnp.bfloat16)


def shard_levels(stream_key, shape, shards, least, largest):
    level = 1.0
    for dim, parts in shards:
        draws = jax.random.uniform(jax.random.fold_in(jax.random.fold_in(stream_key, 6), dim), (parts,), jnp.float32, least / len(shards), largest / len(shards))
        level = level * jnp.repeat(jnp.exp(draws), shape[dim] // parts).reshape((-1,) + (1,) * (len(shape) - 1 - dim))
    return level


def gaussian(own_key, shape, spread, bound, cuts=(), kind=jnp.bfloat16):
    factor_of = shard_levels(own_key, shape, cuts, -0.22, 0.18) if cuts else 1.0
    values = jax.random.normal(own_key, shape, jnp.float32) * spread * factor_of
    return jnp.minimum(jnp.maximum(values, -bound), bound).astype(kind)


def setup_inputs(seed: int = 0, part: int = 0) -> dict:
    arg_keys = jax.random.split(jax.random.key(seed), 13)
    part_splits = jax.random.split(jax.random.fold_in(arg_keys[12], part), 13)
    tokens = gaussian(part_splits[0], (TOKENS, D), 1.0, 6.0, ((0, 32), (1, 4)))
    norm_gain = jnp.clip(1.0 + 0.18 * jax.random.normal(arg_keys[1], (D,), jnp.float32), 0.1, 1.9)
    pool_weight = gaussian(arg_keys[2], (GROUPS, GROUP_CH, GROUP_CH), GROUP_CH ** -0.5, 0.25, ((0, 4),))
    pool_scale = jnp.clip(1.0 + 0.18 * jax.random.normal(arg_keys[3], (D,), jnp.float32), 0.1, 1.9)
    query_weight = draw_query_weight(jax.random.fold_in(arg_keys[12], 71), part)
    gate_weight = gaussian(arg_keys[5], (D, HEADS), D ** -0.5, 0.125)
    key_weight = gaussian(arg_keys[6], (D, HEADS * HD), D ** -0.5, 0.125, ((1, 4),))
    value_weight = gaussian(arg_keys[7], (D, HEADS * HD), D ** -0.5, 0.125, ((1, 4),))
    out_weight = gaussian(arg_keys[8], (HEADS * HD, D), (HEADS * HD) ** -0.5, 0.1875, ((1, 4),))
    passage_gain = jnp.clip(1.0 + 0.18 * jax.random.normal(arg_keys[9], (D,), jnp.float32), 0.1, 1.9)
    passage_store = gaussian(part_splits[10], (PASSAGES, PLEN, D), 1.0, 6.0, ((0, 32),))
    passage_ids = draw_passage_ids(jax.random.fold_in(jax.random.fold_in(arg_keys[12], part), 71), part)
    return {"tokens": tokens, "norm_gain": norm_gain, "pool_weight": pool_weight, "pool_scale": pool_scale, "query_weight": query_weight, "gate_weight": gate_weight, "key_weight": key_weight, "value_weight": value_weight, "out_weight": out_weight, "passage_gain": passage_gain, "passage_store": passage_store, "passage_ids": passage_ids}


epsilon = 1e-06

def rms_norm(values, gain):
    wide_values = values.astype(jnp.float32)
    inverse = lax.rsqrt(lax.optimization_barrier(jnp.mean(wide_values * wide_values, axis=-1, keepdims=True)) + epsilon)
    return (wide_values * inverse * gain).astype(jnp.bfloat16)

def reference(tokens, norm_gain, pool_weight, pool_scale, query_weight, gate_weight, key_weight, value_weight, out_weight, passage_gain, passage_store, passage_ids):
    normed = rms_norm(tokens, norm_gain)
    sequences = TOKENS // SEQ_LEN
    channels = D // GROUPS
    grouped = normed.astype(jnp.float32).reshape(sequences, SEQ_LEN, GROUPS, channels)
    running = jnp.cumsum(grouped, axis=1)
    position = jnp.arange(SEQ_LEN)
    pieces = []
    for group_index in range(GROUPS):
        window = 2 ** (group_index + 1)
        current = running[:, :, group_index]
        lagged = jnp.pad(current, ((0, 0), (window, 0), (0, 0)))[:, :SEQ_LEN]
        divisor = jnp.minimum(position + 1, window).astype(jnp.float32)[None, :, None]
        pieces.append((current - lagged) / divisor - grouped[:, :, group_index])
    pooled = jnp.stack(pieces, axis=2).astype(jnp.bfloat16).reshape(TOKENS, GROUPS, channels)
    mixing = jnp.einsum('tgc,gcd->tgd', pooled.astype(jnp.float32), pool_weight.astype(jnp.float32)).reshape(TOKENS, D) * pool_scale
    queries = jnp.dot(normed, query_weight, preferred_element_type=jnp.float32).astype(jnp.bfloat16)
    gating = jax.nn.sigmoid(jnp.dot(normed, gate_weight, preferred_element_type=jnp.float32))
    query_blocks = queries.reshape(BLOCKS, BLK, HEADS, HD)
    gate_blocks = gating.reshape(BLOCKS, BLK, HEADS)

    def one_block(inputs):
        block_queries, block_gates, block_ids = inputs
        fetched = jnp.take(passage_store, block_ids, axis=0).reshape(NPB * PLEN, D)
        passage_rows = rms_norm(fetched, passage_gain)
        key_rows = jnp.dot(passage_rows, key_weight, preferred_element_type=jnp.float32).astype(jnp.bfloat16).reshape(NPB * PLEN, HEADS, HD)
        values = jnp.dot(passage_rows, value_weight, preferred_element_type=jnp.float32).astype(jnp.bfloat16).reshape(NPB * PLEN, HEADS, HD)
        scores = jnp.einsum('qhd,khd->hqk', block_queries.astype(jnp.float32), key_rows.astype(jnp.float32)) * HD ** (-0.5)
        row_max = lax.optimization_barrier(jnp.max(scores, axis=-1, keepdims=True))
        weights = jnp.exp(scores - row_max)
        probabilities = (weights / lax.optimization_barrier(jnp.sum(weights, axis=-1, keepdims=True))).astype(jnp.bfloat16)
        attended = jnp.einsum('hqk,khd->qhd', probabilities.astype(jnp.float32), values.astype(jnp.float32))
        return (attended * block_gates[:, :, None]).astype(jnp.bfloat16).reshape(BLK, HEADS * HD)
    head_out = lax.map(one_block, (query_blocks, gate_blocks, passage_ids)).reshape(TOKENS, HEADS * HD)
    crossed = jnp.dot(head_out, out_weight, preferred_element_type=jnp.float32)
    return (mixing + crossed).astype(jnp.bfloat16)
```

```python
import jax
import jax.numpy as jnp
from jax import lax
from jax.experimental import pallas as pl
from jax.experimental.pallas import tpu as pltpu
from jax.sharding import PartitionSpec as P

HD = 128
GROUPS = 4
SEQ_LEN = 256
BLK = 128
NPB = 4
PLEN = 64
P_DEV = 24

epsilon = 1e-06
PROJ_ROWS = 256
PACK_SLOTS = 16
OUT_ROWS = 256


def project_kernel(store_ref, gain_ref, key_ref, value_ref, out_ref):
    wide = store_ref[...].astype(jnp.float32)
    inverse = lax.rsqrt(jnp.mean(wide * wide, axis=-1, keepdims=True) + epsilon)
    rows = (wide * inverse * gain_ref[...]).astype(jnp.bfloat16)
    half = key_ref.shape[1]
    keys = jnp.dot(rows, key_ref[...], preferred_element_type=jnp.float32)
    values = jnp.dot(rows, value_ref[...], preferred_element_type=jnp.float32)
    out_ref[:, :half] = keys.astype(jnp.bfloat16)
    out_ref[:, half:] = values.astype(jnp.bfloat16)


def project_store(store, gain, key_weight, value_weight):
    rows, width = store.shape
    head_width = key_weight.shape[1]
    return pl.pallas_call(
        project_kernel,
        grid=(rows // PROJ_ROWS,),
        in_specs=[
            pl.BlockSpec((PROJ_ROWS, width), lambda i: (i, 0)),
            pl.BlockSpec((1, width), lambda i: (0, 0)),
            pl.BlockSpec((width, head_width), lambda i: (0, 0)),
            pl.BlockSpec((width, head_width), lambda i: (0, 0)),
        ],
        out_specs=pl.BlockSpec((PROJ_ROWS, 2 * head_width), lambda i: (i, 0)),
        out_shape=jax.ShapeDtypeStruct((rows, 2 * head_width), jnp.bfloat16),
        name="project_store",
    )(store, gain.reshape(1, width), key_weight, value_weight)


def pack_kernel(index_ref, store_ref, out_ref):
    count = out_ref.shape[0]
    first = pl.program_id(0) * count
    for slot in range(count):
        out_ref[slot] = store_ref[index_ref[first + slot]]


def pack_slots(index, store):
    slots = index.shape[0]
    _, rows, width = store.shape
    return pl.pallas_call(
        pack_kernel,
        grid_spec=pltpu.PrefetchScalarGridSpec(
            num_scalar_prefetch=1,
            grid=(slots // PACK_SLOTS,),
            in_specs=[pl.BlockSpec(store.shape, lambda i, s: (0, 0, 0))],
            out_specs=pl.BlockSpec((PACK_SLOTS, rows, width), lambda i, s: (i, 0, 0)),
        ),
        out_shape=jax.ShapeDtypeStruct((slots, rows, width), jnp.bfloat16),
        name="pack_slots",
    )(index, store)


def attend_kernel(first, index_ref, query_ref, gate_ref, table_ref, out_ref):
    blocks = out_ref.shape[0] // BLK
    width = query_ref.shape[1]
    for block in range(blocks):
        rows = slice(block * BLK, (block + 1) * BLK)
        slots = [index_ref[(first + block) * NPB + part] for part in range(NPB)]
        for head in range(width // HD):
            cols = slice(head * HD, (head + 1) * HD)
            late = slice(width + head * HD, width + (head + 1) * HD)
            keys = jnp.concatenate([table_ref[slot, :, cols] for slot in slots], axis=0)
            values = jnp.concatenate([table_ref[slot, :, late] for slot in slots], axis=0)
            scores = lax.dot_general(
                query_ref[rows, cols],
                keys,
                (((1,), (1,)), ((), ())),
                preferred_element_type=jnp.float32,
            ) * HD ** (-0.5)
            weights = jnp.exp(scores - jnp.max(scores, axis=-1, keepdims=True))
            total = jnp.sum(weights, axis=-1, keepdims=True)
            probabilities = (weights / total).astype(jnp.bfloat16)
            attended = jnp.dot(probabilities, values, preferred_element_type=jnp.float32)
            out_ref[rows, cols] = (attended * gate_ref[rows, head : head + 1]).astype(jnp.bfloat16)


def attend(index, queries, gates, table, half):
    rows, width = queries.shape
    rows = rows // 2
    first = half * rows // BLK
    return pl.pallas_call(
        lambda *refs: attend_kernel(first, *refs),
        grid_spec=pltpu.PrefetchScalarGridSpec(
            num_scalar_prefetch=1,
            grid=(1,),
            in_specs=[
                pl.BlockSpec((rows, width), lambda i, s: (half, 0)),
                pl.BlockSpec((rows, gates.shape[1]), lambda i, s: (half, 0)),
                pl.BlockSpec(table.shape, lambda i, s: (0, 0, 0)),
            ],
            out_specs=pl.BlockSpec((rows, width), lambda i, s: (0, 0)),
        ),
        out_shape=jax.ShapeDtypeStruct((rows, width), jnp.bfloat16),
        name="attend",
    )(index, queries, gates, table)


def add_products_kernel(*refs):
    base_ref, out_ref = refs[0], refs[-1]
    pairs = refs[1:-1]
    count = len(pairs) // 2
    total = base_ref[...]
    for k in range(count):
        total = total + jnp.dot(
            pairs[k][...], pairs[count + k][...], preferred_element_type=jnp.float32
        )
    out_ref[...] = total.astype(out_ref.dtype)


def add_products(base, pieces, weights, dtype):
    rows, width = base.shape
    steps = rows // OUT_ROWS
    narrow = pieces[0].shape[1]
    return pl.pallas_call(
        add_products_kernel,
        grid=(steps,),
        in_specs=[pl.BlockSpec((OUT_ROWS, width), lambda i: (i, 0))]
        + [pl.BlockSpec((OUT_ROWS, narrow), lambda i: (i, 0))] * len(pieces)
        + [pl.BlockSpec((narrow, width), lambda i: (0, 0))] * len(weights),
        out_specs=pl.BlockSpec((OUT_ROWS, width), lambda i: (i, 0)),
        out_shape=jax.ShapeDtypeStruct((rows, width), dtype),
        name="add_products",
    )(base, *pieces, *weights)


def per_device(
    tokens,
    norm_gain,
    pool_weight,
    pool_scale,
    query_weight,
    gate_weight,
    key_weight,
    value_weight,
    out_weight,
    passage_gain,
    passage_store,
    passage_ids,
):
    head_index = lax.axis_index("tp")
    tp_count = lax.axis_size("tp")
    tok_rows, width_local = tokens.shape
    full_width = width_local * tp_count
    local_heads = query_weight.shape[1] // HD
    store_rows = passage_store.shape[0] * PLEN

    flat_ids = passage_ids.reshape(-1)
    asked_count = flat_ids.shape[0]
    st_count = lax.axis_size("st")
    capacity = max(2, (asked_count + st_count - 1) // st_count)
    owners = flat_ids // P_DEV
    local_index = flat_ids % P_DEV
    order_index = jnp.arange(asked_count, dtype=jnp.int32)
    earlier = (owners[None, :] == owners[:, None]) & (order_index[None, :] < order_index[:, None])
    slot_index = jnp.sum(earlier.astype(jnp.int32), axis=1)
    position_flat = owners * capacity + slot_index
    slot_range = jnp.arange(st_count * capacity, dtype=jnp.int32)
    request_table = jnp.sum(
        jnp.where(position_flat[None, :] == slot_range[:, None], local_index[None, :], 0), axis=1
    )
    request_table = request_table.reshape(st_count, capacity)
    asked = lax.all_to_all(request_table, "st", split_axis=0, concat_axis=0, tiled=True)

    projected = project_store(
        passage_store.reshape(store_rows, full_width), passage_gain, key_weight, value_weight
    )
    width_both = projected.shape[1]
    packed = pack_slots(asked.reshape(-1), projected.reshape(-1, PLEN, width_both))
    returned = lax.all_to_all(
        packed.reshape(st_count, capacity * PLEN, width_both),
        "st",
        split_axis=0,
        concat_axis=0,
        tiled=True,
    ).reshape(st_count * capacity, PLEN, width_both)

    wide_tokens = tokens.astype(jnp.float32)
    square_sums = lax.psum(jnp.sum(wide_tokens * wide_tokens, axis=1), "tp")
    inverse = lax.rsqrt(square_sums / full_width + epsilon)
    gain_local = lax.dynamic_slice_in_dim(norm_gain, head_index * width_local, width_local)
    normed = (wide_tokens * inverse[:, None] * gain_local[None, :]).astype(jnp.bfloat16)
    columns = lax.all_gather(normed, "tp", axis=1, tiled=True)

    sequences = tok_rows // SEQ_LEN
    window = jnp.left_shift(jnp.int32(2), head_index)
    grouped = normed.astype(jnp.float32).reshape(sequences, SEQ_LEN, width_local)
    total = grouped
    for level in range(GROUPS):
        shift = 2**level
        moved = jnp.pad(total, ((0, 0), (shift, 0), (0, 0)))[:, :SEQ_LEN]
        total = jnp.where(level <= head_index, total + moved, total)
    position = jnp.arange(SEQ_LEN, dtype=jnp.int32)
    divisor = jnp.minimum(position + 1, window).astype(jnp.float32)
    pooled = (
        (total / divisor[None, :, None] - grouped)
        .astype(jnp.bfloat16)
        .reshape(tok_rows, width_local)
    )
    base = (
        jnp.dot(pooled, pool_weight[0], preferred_element_type=jnp.float32) * pool_scale[None, :]
    )

    gate_columns = lax.dynamic_slice_in_dim(
        gate_weight, head_index * local_heads, local_heads, axis=1
    )
    query_sum = jnp.dot(columns, query_weight, preferred_element_type=jnp.float32)
    gate_sum = jnp.dot(columns, gate_columns, preferred_element_type=jnp.float32)
    queries = query_sum.astype(jnp.bfloat16)
    gating = jax.nn.sigmoid(gate_sum)

    rows_of = out_weight.reshape(tp_count, local_heads * HD, width_local)
    weights = [
        lax.dynamic_index_in_dim(rows_of, (head_index + place) % tp_count, 0, keepdims=False)
        for place in (0, tp_count - 1, 1, 2)
    ]
    queries, gating, base, weights = lax.optimization_barrier((queries, gating, base, weights))

    up = [(i, (i + 1) % tp_count) for i in range(tp_count)]
    down = [(i, (i - 1) % tp_count) for i in range(tp_count)]
    low = attend(position_flat, queries, gating, returned, 0)
    low_before = lax.ppermute(low, "tp", up)
    high = attend(position_flat, queries, gating, returned, 1)
    high_after = lax.ppermute(high, "tp", down)
    high_before = lax.ppermute(high, "tp", up)
    low_after = lax.ppermute(low, "tp", down)
    low_far = lax.ppermute(low_before, "tp", up)
    high_far = lax.ppermute(high_after, "tp", down)
    half = tok_rows // 2
    sides = ((low, low_before, low_after, low_far), (high, high_before, high_after, high_far))
    outs = []
    for side, (own, before, after, far) in enumerate(sides):
        part = base[side * half : (side + 1) * half]
        part = add_products(part, (own, before, after), weights[:3], jnp.float32)
        outs.append(add_products(part, (far,), weights[3:], jnp.bfloat16))
    return jnp.concatenate(outs, axis=0)


def solution(mesh):
    in_specs = (
        P(("grp", "st"), "tp"),
        P(),
        P("tp", None, None),
        P("tp"),
        P(None, "tp"),
        P(),
        P(None, "tp"),
        P(None, "tp"),
        P(None, "tp"),
        P(),
        P(("grp", "st"), None, None),
        P(("grp", "st"), None),
    )
    out_specs = P(("grp", "st"), "tp")
    return jax.shard_map(
        per_device, mesh=mesh, in_specs=in_specs, out_specs=out_specs, check_vma=False
    )
```

```python
import jax
import jax.numpy as jnp
from jax import lax
from jax.experimental import pallas as pl
from jax.experimental.pallas import tpu as pltpu
from jax.sharding import PartitionSpec as P

HD = 128
GROUPS = 4
SEQ_LEN = 256
BLK = 128
NPB = 4
PLEN = 64

epsilon = 1e-06
TILE = 8
SELECT_READERS = 4
OUT_ROWS = 256


def spread_kernel(store_ref, gain_ref, key_ref, value_ref, order_ref, out_ref):
    passages, tile, width = store_ref.shape
    wide = store_ref[...].astype(jnp.float32).reshape(passages * tile, width)
    inverse = lax.rsqrt(jnp.mean(wide * wide, axis=-1, keepdims=True) + epsilon)
    rows = (wide * gain_ref[...]).astype(jnp.bfloat16)
    half = key_ref.shape[1]
    for part, weight_ref in enumerate((key_ref, value_ref)):
        product = jnp.dot(rows, weight_ref[...], preferred_element_type=jnp.float32)
        product = (product * inverse).astype(jnp.bfloat16)
        turned = jnp.dot(order_ref[...], product, preferred_element_type=jnp.float32)
        turned = turned.reshape(tile, passages, half).astype(jnp.bfloat16)
        out_ref[:, :, part * half : (part + 1) * half] = turned


def spread_store(store, gain, key_weight, value_weight, holders):
    passages, length, width = store.shape
    head_width = key_weight.shape[1]
    rows = passages * TILE
    spot = jnp.arange(rows, dtype=jnp.int32)
    wanted = (spot % passages) * TILE + spot // passages
    order = (wanted[:, None] == spot[None, :]).astype(jnp.bfloat16)
    groups = holders // TILE
    return pl.pallas_call(
        spread_kernel,
        grid=(length // TILE,),
        in_specs=[
            pl.BlockSpec((passages, TILE, width), lambda i: (0, i, 0)),
            pl.BlockSpec((1, width), lambda i: (0, 0)),
            pl.BlockSpec((width, head_width), lambda i: (0, 0)),
            pl.BlockSpec((width, head_width), lambda i: (0, 0)),
            pl.BlockSpec((rows, rows), lambda i: (0, 0)),
        ],
        out_specs=pl.BlockSpec(
            (TILE, passages, 2 * head_width), lambda i: (i % groups, i // groups, 0)
        ),
        out_shape=jax.ShapeDtypeStruct(
            (holders, passages * length // holders, 2 * head_width), jnp.bfloat16
        ),
        name="spread_store",
    )(store, gain.reshape(1, width), key_weight, value_weight, order)


def select_kernel(wanted_ref, table_ref, out_ref):
    count = wanted_ref.shape[0]
    spot = lax.broadcasted_iota(jnp.int32, (count, table_ref.shape[0]), 1)
    chosen = jnp.where(spot == wanted_ref[...], 1.0, 0.0).astype(jnp.bfloat16)
    out_ref[...] = jnp.dot(chosen, table_ref[...], preferred_element_type=jnp.float32).astype(
        jnp.bfloat16
    )


def select_rows(wanted, table, step_rows):
    rows = wanted.shape[0]
    width = table.shape[1]
    return pl.pallas_call(
        select_kernel,
        grid=(rows // step_rows,),
        in_specs=[
            pl.BlockSpec((step_rows, 1), lambda i: (i, 0)),
            pl.BlockSpec(table.shape, lambda i: (0, 0)),
        ],
        out_specs=pl.BlockSpec((step_rows, width), lambda i: (i, 0)),
        out_shape=jax.ShapeDtypeStruct((rows, width), jnp.bfloat16),
        name="select_rows",
    )(wanted, table)


def attend_kernel(query_ref, gate_ref, table_ref, out_ref):
    holders, tile, both = table_ref.shape
    width = query_ref.shape[1]
    table = table_ref[...].astype(jnp.float32).reshape(holders * tile, both)
    table = table.astype(jnp.bfloat16)
    for head in range(width // HD):
        cols = slice(head * HD, (head + 1) * HD)
        late = slice(width + head * HD, width + (head + 1) * HD)
        scores = lax.dot_general(
            query_ref[:, cols],
            table[:, cols],
            (((1,), (1,)), ((), ())),
            preferred_element_type=jnp.float32,
        ) * HD ** (-0.5)
        weights = jnp.exp(scores - jnp.max(scores, axis=-1, keepdims=True))
        total = jnp.sum(weights, axis=-1, keepdims=True)
        probabilities = (weights / total).astype(jnp.bfloat16)
        attended = jnp.dot(probabilities, table[:, late], preferred_element_type=jnp.float32)
        out_ref[:, cols] = (attended * gate_ref[:, head : head + 1]).astype(jnp.bfloat16)


def attend(queries, gates, table, half):
    rows, width = queries.shape
    rows = rows // 2
    blocks = rows // BLK
    first = half * blocks
    holders, _, both = table.shape
    return pl.pallas_call(
        attend_kernel,
        grid=(blocks,),
        in_specs=[
            pl.BlockSpec((BLK, width), lambda i: (first + i, 0)),
            pl.BlockSpec((BLK, gates.shape[1]), lambda i: (first + i, 0)),
            pl.BlockSpec((holders, TILE, both), lambda i: (0, first + i, 0)),
        ],
        out_specs=pl.BlockSpec((BLK, width), lambda i: (i, 0)),
        out_shape=jax.ShapeDtypeStruct((rows, width), jnp.bfloat16),
        name="attend",
    )(queries, gates, table)


def finish_kernel(halves, weight_ref, base_ref, *refs):
    out_ref = refs[-1]
    pieces = refs[:-1]
    count = len(pieces) // halves
    step = pl.program_id(0)
    each = pl.num_programs(0) // halves
    for half in range(halves):

        @pl.when(step // each == half)
        def _():
            total = base_ref[...]
            for k in range(count):
                total = total + jnp.dot(
                    pieces[half * count + k][...], weight_ref[k], preferred_element_type=jnp.float32
                )
            out_ref[...] = total.astype(out_ref.dtype)


def finish(base, sides, weights):
    rows, width = base.shape
    halves = len(sides)
    each = rows // OUT_ROWS // halves
    narrow = sides[0][0].shape[1]

    def spec(half):
        return pl.BlockSpec(
            (OUT_ROWS, narrow), lambda i: (jnp.clip(i - half * each, 0, each - 1), 0)
        )

    return pl.pallas_call(
        lambda *refs: finish_kernel(halves, *refs),
        grid=(each * halves,),
        in_specs=[
            pl.BlockSpec(weights.shape, lambda i: (0, 0, 0)),
            pl.BlockSpec((OUT_ROWS, width), lambda i: (i, 0)),
        ]
        + [spec(half) for half in range(halves) for _ in sides[half]],
        out_specs=pl.BlockSpec((OUT_ROWS, width), lambda i: (i, 0)),
        out_shape=jax.ShapeDtypeStruct((rows, width), jnp.bfloat16),
        name="finish",
    )(weights, base, *[piece for side in sides for piece in side])


def per_device(
    tokens,
    norm_gain,
    pool_weight,
    pool_scale,
    query_weight,
    gate_weight,
    key_weight,
    value_weight,
    out_weight,
    passage_gain,
    passage_store,
    passage_ids,
):
    head_index = lax.axis_index("tp")
    tp_count = lax.axis_size("tp")
    tok_rows, width_local = tokens.shape
    full_width = width_local * tp_count
    local_heads = query_weight.shape[1] // HD
    st_count = lax.axis_size("st")
    passages = passage_store.shape[0]
    shares = PLEN // st_count
    spread = spread_store(passage_store, passage_gain, key_weight, value_weight, st_count)
    width_both = spread.shape[2]
    held = lax.all_to_all(spread, "st", split_axis=0, concat_axis=0, tiled=True)

    all_ids = lax.all_gather(passage_ids.reshape(-1), "st", axis=0)
    all_ids = all_ids.reshape(st_count, -1, 1, NPB)
    owners = lax.div(all_ids, jnp.int32(passages))
    share = jnp.arange(shares, dtype=jnp.int32)[None, None, :, None]
    wanted = owners * (shares * passages) + share * passages + (all_ids - owners * passages)
    packed = select_rows(
        wanted.reshape(-1, 1),
        held.reshape(-1, width_both),
        SELECT_READERS * NPB * shares * (tok_rows // BLK),
    )
    returned = lax.all_to_all(
        packed.reshape(st_count, -1, width_both), "st", split_axis=0, concat_axis=0, tiled=True
    )

    wide_tokens = tokens.astype(jnp.float32)
    square_sums = lax.psum(jnp.sum(wide_tokens * wide_tokens, axis=1), "tp")
    inverse = lax.rsqrt(square_sums / full_width + epsilon)
    gain_local = lax.dynamic_slice_in_dim(norm_gain, head_index * width_local, width_local)
    normed = (wide_tokens * inverse[:, None] * gain_local[None, :]).astype(jnp.bfloat16)
    columns = lax.all_gather(normed, "tp", axis=1, tiled=True)

    sequences = tok_rows // SEQ_LEN
    window = jnp.left_shift(jnp.int32(2), head_index)
    grouped = normed.astype(jnp.float32).reshape(sequences, SEQ_LEN, width_local)
    total = grouped
    for level in range(GROUPS):
        shift = 2**level
        moved = jnp.pad(total, ((0, 0), (shift, 0), (0, 0)))[:, :SEQ_LEN]
        total = jnp.where(level <= head_index, total + moved, total)
    position = jnp.arange(SEQ_LEN, dtype=jnp.int32)
    divisor = jnp.minimum(position + 1, window).astype(jnp.float32)
    pooled = (
        (total / divisor[None, :, None] - grouped)
        .astype(jnp.bfloat16)
        .reshape(tok_rows, width_local)
    )
    base = (
        jnp.dot(pooled, pool_weight[0], preferred_element_type=jnp.float32) * pool_scale[None, :]
    )

    gate_columns = lax.dynamic_slice_in_dim(
        gate_weight, head_index * local_heads, local_heads, axis=1
    )
    query_sum = jnp.dot(columns, query_weight, preferred_element_type=jnp.float32)
    gate_sum = jnp.dot(columns, gate_columns, preferred_element_type=jnp.float32)
    queries = query_sum.astype(jnp.bfloat16)
    gating = jax.nn.sigmoid(gate_sum)

    rows_of = out_weight.reshape(tp_count, local_heads * HD, width_local)
    turned = (head_index + jnp.array([0, tp_count - 1, 1, 2], dtype=jnp.int32)) % tp_count
    weights = jnp.take(rows_of, turned, axis=0, mode="clip")
    queries, gating, base, weights = lax.optimization_barrier((queries, gating, base, weights))

    up = [(i, (i + 1) % tp_count) for i in range(tp_count)]
    down = [(i, (i - 1) % tp_count) for i in range(tp_count)]
    low = attend(queries, gating, returned, 0)
    low_before = lax.ppermute(low, "tp", up)
    low_after = lax.ppermute(low, "tp", down)
    high = attend(queries, gating, returned, 1)
    high_before = lax.ppermute(high, "tp", up)
    high_after = lax.ppermute(high, "tp", down)
    low_far = lax.ppermute(low_before, "tp", up)
    high_far = lax.ppermute(high_after, "tp", down)
    sides = ((low, low_before, low_after, low_far), (high, high_before, high_after, high_far))
    return finish(base, sides, weights)


def solution(mesh):
    in_specs = (
        P(("grp", "st"), "tp"),
        P(),
        P("tp", None, None),
        P("tp"),
        P(None, "tp"),
        P(),
        P(None, "tp"),
        P(None, "tp"),
        P(None, "tp"),
        P(),
        P(("grp", "st"), None, None),
        P(("grp", "st"), None),
    )
    out_specs = P(("grp", "st"), "tp")
    return jax.shard_map(
        per_device, mesh=mesh, in_specs=in_specs, out_specs=out_specs, check_vma=False
    )
```

```python
import jax
import jax.numpy as jnp
from jax import lax
from jax.experimental import pallas as pl
from jax.experimental.pallas import tpu as pltpu
from jax.sharding import PartitionSpec as P

HD = 128
GROUPS = 4
SEQ_LEN = 256
BLK = 128
NPB = 4
PLEN = 64

epsilon = 1e-06
LANES = 128
TILE = 8
SHARE_ROWS = 16
SELECT_READERS = 8
OUT_ROWS = 256
whole = pl.BlockSpec(memory_space=pltpu.VMEM)


def spread_kernel(ids_ref, store_ref, gain_ref, key_ref, value_ref, out_ref, order_ref):
    step = pl.program_id(0)
    passages, span, width = store_ref.shape
    rows = passages * span
    holders = out_ref.shape[0]
    groups = holders // span
    shares = pl.num_programs(0) // groups
    body = shares * passages

    @pl.when(step == 0)
    def _():
        spot = lax.broadcasted_iota(jnp.int32, (rows, rows), 0)
        holder = lax.div(spot, jnp.int32(passages))
        wanted = (spot - holder * passages) * span + holder
        other = lax.broadcasted_iota(jnp.int32, (rows, rows), 1)
        order_ref[...] = jnp.where(wanted == other, 1.0, 0.0).astype(jnp.bfloat16)
        line = lax.broadcasted_iota(jnp.int32, (TILE, LANES), 0)
        lane = lax.broadcasted_iota(jnp.int32, (TILE, LANES), 1)
        share = lax.shift_right_logical(line, 2)
        part_of = line - share * NPB
        blocks = ids_ref.shape[0]
        tile = jnp.zeros((TILE, LANES), jnp.int32)
        for block in range(blocks):
            for part in range(NPB):
                name = ids_ref[block, part]
                owner = lax.div(name, jnp.int32(passages))
                inside = name - owner * passages
                here = part_of == part
                tile = jnp.where(here & (lane == block), owner, tile)
                tile = jnp.where(here & (lane == blocks + block), inside + share * passages, tile)
        tile = tile.astype(jnp.float32).astype(jnp.bfloat16)
        out_ref[:, out_ref.shape[1] - TILE :, :] = jnp.broadcast_to(tile, (holders, TILE, LANES))

    wide = store_ref[...].astype(jnp.float32).reshape(rows, width)
    inverse = lax.rsqrt(jnp.mean(wide * wide, axis=-1, keepdims=True) + epsilon)
    scaled = (wide * gain_ref[...]).astype(jnp.bfloat16)
    first = pl.multiple_of((step % groups) * span, span)
    offset = (step // groups) * passages
    chunks = key_ref.shape[1] // LANES
    for half, weight_ref in enumerate((key_ref, value_ref)):
        product = jnp.dot(scaled, weight_ref[...], preferred_element_type=jnp.float32)
        product = (product * inverse).astype(jnp.bfloat16)
        turned = jnp.dot(order_ref[...], product, preferred_element_type=jnp.float32)
        turned = turned.reshape(span, passages, chunks * LANES).astype(jnp.bfloat16)
        for chunk in range(chunks):
            start = pl.multiple_of((half * chunks + chunk) * body + offset, TILE)
            out_ref[pl.ds(first, span), pl.ds(start, passages), :] = turned[
                :, :, chunk * LANES : (chunk + 1) * LANES
            ]


def spread_store(ids, store, gain, key_weight, value_weight, holders):
    passages, length, width = store.shape
    head_width = key_weight.shape[1]
    rows = passages * SHARE_ROWS
    per_holder = passages * length // holders * (2 * head_width // LANES) + TILE
    return pl.pallas_call(
        spread_kernel,
        grid_spec=pltpu.PrefetchScalarGridSpec(
            num_scalar_prefetch=1,
            grid=(length // SHARE_ROWS,),
            in_specs=[
                pl.BlockSpec((passages, SHARE_ROWS, width), lambda i, s: (0, i, 0)),
                pl.BlockSpec((1, width), lambda i, s: (0, 0)),
                pl.BlockSpec((width, head_width), lambda i, s: (0, 0)),
                pl.BlockSpec((width, head_width), lambda i, s: (0, 0)),
            ],
            out_specs=pl.BlockSpec((holders, per_holder, LANES), lambda i, s: (0, 0, 0)),
            scratch_shapes=[pltpu.VMEM((rows, rows), jnp.bfloat16)],
        ),
        out_shape=jax.ShapeDtypeStruct((holders, per_holder, LANES), jnp.bfloat16),
        name="spread_store",
    )(ids, store, gain.reshape(1, width), key_weight, value_weight)


def select_kernel(blocks, held_ref, out_ref, table_ref):
    step = pl.program_id(0)
    owners = held_ref.shape[0]
    chunks = table_ref.shape[1] // LANES
    body = table_ref.shape[0] // owners

    @pl.when(step == 0)
    def _():
        for owner in range(owners):
            for chunk in range(chunks):
                table_ref[
                    owner * body : (owner + 1) * body, chunk * LANES : (chunk + 1) * LANES
                ] = held_ref[owner, chunk * body : (chunk + 1) * body, :]

    spot = lax.broadcasted_iota(jnp.int32, (TILE, table_ref.shape[0]), 1).astype(jnp.float32)
    chosen = []
    for reader in range(SELECT_READERS):
        tile = held_ref[step * SELECT_READERS + reader, chunks * body :, :].astype(jnp.float32)
        for block in range(blocks):
            wanted = tile[:, block : block + 1] * float(body)
            wanted = wanted + tile[:, blocks + block : blocks + block + 1]
            chosen.append(jnp.where(spot == wanted, 1.0, 0.0))
    chosen = jnp.concatenate(chosen, axis=0).astype(jnp.bfloat16)
    out_ref[...] = jnp.dot(chosen, table_ref[...], preferred_element_type=jnp.float32).astype(
        jnp.bfloat16
    )


def select_rows(held, blocks, body, width):
    owners = held.shape[0]
    step_rows = SELECT_READERS * blocks * TILE
    return pl.pallas_call(
        lambda *refs: select_kernel(blocks, *refs),
        grid=(owners // SELECT_READERS,),
        in_specs=[whole],
        out_specs=pl.BlockSpec((step_rows, width), lambda i: (i, 0)),
        out_shape=jax.ShapeDtypeStruct((owners * blocks * TILE, width), jnp.bfloat16),
        scratch_shapes=[pltpu.VMEM((owners * body, width), jnp.bfloat16)],
        name="select_rows",
    )(held)


def attend_kernel(half, query_ref, gate_ref, table_ref, out_ref):
    holders, _, both = table_ref.shape
    width = query_ref.shape[1]
    rows = out_ref.shape[0]
    for block in range(rows // BLK):
        place = half * rows // BLK + block
        mine = slice(place * BLK, (place + 1) * BLK)
        table = table_ref[:, place * TILE : (place + 1) * TILE, :].astype(jnp.float32)
        table = table.reshape(holders * TILE, both).astype(jnp.bfloat16)
        for head in range(width // HD):
            cols = slice(head * HD, (head + 1) * HD)
            late = slice(width + head * HD, width + (head + 1) * HD)
            scores = lax.dot_general(
                query_ref[mine, cols],
                table[:, cols],
                (((1,), (1,)), ((), ())),
                preferred_element_type=jnp.float32,
            ) * HD ** (-0.5)
            weights = jnp.exp(scores - jnp.max(scores, axis=-1, keepdims=True))
            total = jnp.sum(weights, axis=-1, keepdims=True)
            probabilities = (weights * (1.0 / total)).astype(jnp.bfloat16)
            attended = jnp.dot(probabilities, table[:, late], preferred_element_type=jnp.float32)
            out_ref[block * BLK : (block + 1) * BLK, cols] = (
                attended * gate_ref[mine, head : head + 1]
            ).astype(jnp.bfloat16)


def attend(queries, gates, table, half):
    rows, width = queries.shape
    return pl.pallas_call(
        lambda *refs: attend_kernel(half, *refs),
        in_specs=[whole, whole, whole],
        out_specs=whole,
        out_shape=jax.ShapeDtypeStruct((rows // 2, width), jnp.bfloat16),
        name="attend",
    )(queries, gates, table)


def finish_kernel(halves, weight_ref, base_ref, *refs):
    out_ref = refs[-1]
    pieces = refs[:-1]
    count = len(pieces) // halves
    step = pl.program_id(0)
    each = pl.num_programs(0) // halves
    rows = out_ref.shape[0]
    for half in range(halves):

        @pl.when(step // each == half)
        def _():
            total = base_ref[pl.ds(pl.multiple_of(step * rows, rows), rows), :]
            mine = pl.ds(pl.multiple_of((step - half * each) * rows, rows), rows)
            for k in range(count):
                total = total + jnp.dot(
                    pieces[half * count + k][mine, :],
                    weight_ref[k],
                    preferred_element_type=jnp.float32,
                )
            out_ref[...] = total.astype(out_ref.dtype)


def finish(base, sides, weights):
    rows, width = base.shape
    halves = len(sides)
    pieces = [piece for side in sides for piece in side]
    return pl.pallas_call(
        lambda *refs: finish_kernel(halves, *refs),
        grid=(rows // OUT_ROWS,),
        in_specs=[whole] * (2 + len(pieces)),
        out_specs=pl.BlockSpec((OUT_ROWS, width), lambda i: (i, 0)),
        out_shape=jax.ShapeDtypeStruct((rows, width), jnp.bfloat16),
        name="finish",
    )(weights, base, *pieces)


def per_device(
    tokens,
    norm_gain,
    pool_weight,
    pool_scale,
    query_weight,
    gate_weight,
    key_weight,
    value_weight,
    out_weight,
    passage_gain,
    passage_store,
    passage_ids,
):
    head_index = lax.axis_index("tp")
    tp_count = lax.axis_size("tp")
    tok_rows, width_local = tokens.shape
    full_width = width_local * tp_count
    local_heads = query_weight.shape[1] // HD
    st_count = lax.axis_size("st")
    passages = passage_store.shape[0]
    shares = PLEN // st_count
    spread = spread_store(
        passage_ids, passage_store, passage_gain, key_weight, value_weight, st_count
    )
    held = lax.all_to_all(spread, "st", split_axis=0, concat_axis=0, tiled=True)
    width_both = key_weight.shape[1] + value_weight.shape[1]
    packed = select_rows(held, tok_rows // BLK, shares * passages, width_both)
    returned = lax.all_to_all(
        packed.reshape(st_count, -1, width_both), "st", split_axis=0, concat_axis=0, tiled=True
    )

    wide_tokens = tokens.astype(jnp.float32)
    square_sums = lax.psum(jnp.sum(wide_tokens * wide_tokens, axis=1), "tp")
    inverse = lax.rsqrt(square_sums / full_width + epsilon)
    gain_local = lax.dynamic_slice_in_dim(norm_gain, head_index * width_local, width_local)
    normed = (wide_tokens * inverse[:, None] * gain_local[None, :]).astype(jnp.bfloat16)
    columns = lax.all_gather(normed, "tp", axis=1, tiled=True)

    sequences = tok_rows // SEQ_LEN
    window = jnp.left_shift(jnp.int32(2), head_index)
    grouped = normed.astype(jnp.float32).reshape(sequences, SEQ_LEN, width_local)
    total = grouped
    for level in range(GROUPS):
        shift = 2**level
        moved = jnp.pad(total, ((0, 0), (shift, 0), (0, 0)))[:, :SEQ_LEN]
        total = jnp.where(level <= head_index, total + moved, total)
    position = jnp.arange(SEQ_LEN, dtype=jnp.int32)
    divisor = jnp.minimum(position + 1, window).astype(jnp.float32)
    pooled = (
        (total / divisor[None, :, None] - grouped)
        .astype(jnp.bfloat16)
        .reshape(tok_rows, width_local)
    )
    base = (
        jnp.dot(pooled, pool_weight[0], preferred_element_type=jnp.float32) * pool_scale[None, :]
    )

    gate_columns = lax.dynamic_slice_in_dim(
        gate_weight, head_index * local_heads, local_heads, axis=1
    )
    query_sum = jnp.dot(columns, query_weight, preferred_element_type=jnp.float32)
    gate_sum = jnp.dot(columns, gate_columns, preferred_element_type=jnp.float32)
    queries = query_sum.astype(jnp.bfloat16)
    gating = jax.nn.sigmoid(gate_sum)

    rows_of = out_weight.reshape(tp_count, local_heads * HD, width_local)
    turned = (head_index + jnp.array([0, tp_count - 1, 1, 2], dtype=jnp.int32)) % tp_count
    weights = jnp.take(rows_of, turned, axis=0, mode="clip")
    queries, gating, base, weights = lax.optimization_barrier((queries, gating, base, weights))

    up = [(i, (i + 1) % tp_count) for i in range(tp_count)]
    down = [(i, (i - 1) % tp_count) for i in range(tp_count)]
    low = attend(queries, gating, returned, 0)
    low_before = lax.ppermute(low, "tp", up)
    low_after = lax.ppermute(low, "tp", down)
    high = attend(queries, gating, returned, 1)
    high_before = lax.ppermute(high, "tp", up)
    high_after = lax.ppermute(high, "tp", down)
    low_far = lax.ppermute(low_before, "tp", up)
    high_far = lax.ppermute(high_after, "tp", down)
    sides = ((low, low_before, low_after, low_far), (high, high_before, high_after, high_far))
    return finish(base, sides, weights)


def solution(mesh):
    in_specs = (
        P(("grp", "st"), "tp"),
        P(),
        P("tp", None, None),
        P("tp"),
        P(None, "tp"),
        P(),
        P(None, "tp"),
        P(None, "tp"),
        P(None, "tp"),
        P(),
        P(("grp", "st"), None, None),
        P(("grp", "st"), None),
    )
    out_specs = P(("grp", "st"), "tp")
    return jax.shard_map(
        per_device, mesh=mesh, in_specs=in_specs, out_specs=out_specs, check_vma=False
    )
```

```python
import jax
import jax.numpy as jnp
from jax import lax
from jax.experimental import pallas as pl
from jax.experimental.pallas import tpu as pltpu
from jax.sharding import PartitionSpec as P

HD = 128
GROUPS = 4
SEQ_LEN = 256
BLK = 128
NPB = 4
PLEN = 64

epsilon = 1e-06
LANES = 128
TILE = 8
SHARE_ROWS = 16
SELECT_READERS = 8
OUT_ROWS = 256
whole = pl.BlockSpec(memory_space=pltpu.VMEM)


def spread_kernel(ids_ref, store_ref, gain_ref, key_ref, value_ref, out_ref, order_ref):
    step = pl.program_id(0)
    passages, span, width = store_ref.shape
    rows = passages * span
    holders = out_ref.shape[0]
    groups = holders // span
    shares = pl.num_programs(0) // groups
    body = shares * passages

    @pl.when(step == 0)
    def _():
        spot = lax.broadcasted_iota(jnp.int32, (rows, rows), 0)
        holder = lax.div(spot, jnp.int32(passages))
        wanted = (spot - holder * passages) * span + holder
        other = lax.broadcasted_iota(jnp.int32, (rows, rows), 1)
        order_ref[...] = jnp.where(wanted == other, 1.0, 0.0).astype(jnp.bfloat16)
        line = lax.broadcasted_iota(jnp.int32, (TILE, LANES), 0)
        lane = lax.broadcasted_iota(jnp.int32, (TILE, LANES), 1)
        share = lax.shift_right_logical(line, 2)
        part_of = line - share * NPB
        blocks = ids_ref.shape[1]
        tile = jnp.zeros((TILE, LANES), jnp.int32)
        for block in range(blocks):
            for part in range(NPB):
                name = ids_ref[part, block]
                owner = lax.div(name, jnp.int32(passages))
                inside = name - owner * passages
                here = part_of == part
                tile = jnp.where(here & (lane == block), owner, tile)
                tile = jnp.where(here & (lane == blocks + block), inside + share * passages, tile)
        tile = tile.astype(jnp.float32).astype(jnp.bfloat16)
        out_ref[:, out_ref.shape[1] - TILE :, :] = jnp.broadcast_to(tile, (holders, TILE, LANES))

    wide = store_ref[...].astype(jnp.float32).reshape(rows, width)
    inverse = lax.rsqrt(jnp.mean(wide * wide, axis=-1, keepdims=True) + epsilon)
    scaled = (wide * gain_ref[...]).astype(jnp.bfloat16)
    first = pl.multiple_of((step % groups) * span, span)
    offset = (step // groups) * passages
    chunks = key_ref.shape[1] // LANES
    for half, weight_ref in enumerate((key_ref, value_ref)):
        product = jnp.dot(scaled, weight_ref[...], preferred_element_type=jnp.float32)
        product = (product * inverse).astype(jnp.bfloat16)
        turned = jnp.dot(order_ref[...], product, preferred_element_type=jnp.float32)
        turned = turned.reshape(span, passages, chunks * LANES).astype(jnp.bfloat16)
        for chunk in range(chunks):
            start = pl.multiple_of((half * chunks + chunk) * body + offset, TILE)
            out_ref[pl.ds(first, span), pl.ds(start, passages), :] = turned[
                :, :, chunk * LANES : (chunk + 1) * LANES
            ]


def spread_store(ids, store, gain, key_weight, value_weight, holders):
    passages, length, width = store.shape
    head_width = key_weight.shape[1]
    rows = passages * SHARE_ROWS
    per_holder = passages * length // holders * (2 * head_width // LANES) + TILE
    return pl.pallas_call(
        spread_kernel,
        grid_spec=pltpu.PrefetchScalarGridSpec(
            num_scalar_prefetch=1,
            grid=(length // SHARE_ROWS,),
            in_specs=[
                pl.BlockSpec((passages, SHARE_ROWS, width), lambda i, s: (0, i, 0)),
                pl.BlockSpec((1, width), lambda i, s: (0, 0)),
                pl.BlockSpec((width, head_width), lambda i, s: (0, 0)),
                pl.BlockSpec((width, head_width), lambda i, s: (0, 0)),
            ],
            out_specs=pl.BlockSpec((holders, per_holder, LANES), lambda i, s: (0, 0, 0)),
            scratch_shapes=[pltpu.VMEM((rows, rows), jnp.bfloat16)],
        ),
        out_shape=jax.ShapeDtypeStruct((holders, per_holder, LANES), jnp.bfloat16),
        name="spread_store",
    )(ids, store, gain.reshape(1, width), key_weight, value_weight)


def select_kernel(blocks, held_ref, out_ref, table_ref):
    step = pl.program_id(0)
    owners = held_ref.shape[0]
    chunks = table_ref.shape[1] // LANES
    body = table_ref.shape[0] // owners

    @pl.when(step == 0)
    def _():
        for owner in range(owners):
            for chunk in range(chunks):
                table_ref[
                    owner * body : (owner + 1) * body, chunk * LANES : (chunk + 1) * LANES
                ] = held_ref[owner, chunk * body : (chunk + 1) * body, :]

    spot = lax.broadcasted_iota(jnp.int32, (TILE, table_ref.shape[0]), 1).astype(jnp.float32)
    chosen = []
    for reader in range(SELECT_READERS):
        tile = held_ref[step * SELECT_READERS + reader, chunks * body :, :].astype(jnp.float32)
        for block in range(blocks):
            wanted = tile[:, block : block + 1] * float(body)
            wanted = wanted + tile[:, blocks + block : blocks + block + 1]
            chosen.append(jnp.where(spot == wanted, 1.0, 0.0))
    chosen = jnp.concatenate(chosen, axis=0).astype(jnp.bfloat16)
    out_ref[...] = jnp.dot(chosen, table_ref[...], preferred_element_type=jnp.float32).astype(
        jnp.bfloat16
    )


def select_rows(held, blocks, body, width):
    owners = held.shape[0]
    step_rows = SELECT_READERS * blocks * TILE
    return pl.pallas_call(
        lambda *refs: select_kernel(blocks, *refs),
        grid=(owners // SELECT_READERS,),
        in_specs=[whole],
        out_specs=pl.BlockSpec((step_rows, width), lambda i: (i, 0)),
        out_shape=jax.ShapeDtypeStruct((owners * blocks * TILE, width), jnp.bfloat16),
        scratch_shapes=[pltpu.VMEM((owners * body, width), jnp.bfloat16)],
        name="select_rows",
    )(held)


def attend_kernel(query_ref, gate_ref, table_ref, out_ref):
    holders, _, both = table_ref.shape
    width = query_ref.shape[1]
    rows = out_ref.shape[0]
    for block in range(rows // BLK):
        mine = slice(block * BLK, (block + 1) * BLK)
        table = table_ref[:, block * TILE : (block + 1) * TILE, :].astype(jnp.float32)
        table = table.reshape(holders * TILE, both).astype(jnp.bfloat16)
        for head in range(width // HD):
            cols = slice(head * HD, (head + 1) * HD)
            late = slice(width + head * HD, width + (head + 1) * HD)
            scores = lax.dot_general(
                query_ref[mine, cols],
                table[:, cols],
                (((1,), (1,)), ((), ())),
                preferred_element_type=jnp.float32,
            ) * HD ** (-0.5)
            weights = jnp.exp(scores - jnp.max(scores, axis=-1, keepdims=True))
            total = jnp.sum(weights, axis=-1, keepdims=True)
            probabilities = (weights * (1.0 / total)).astype(jnp.bfloat16)
            attended = jnp.dot(probabilities, table[:, late], preferred_element_type=jnp.float32)
            out_ref[mine, cols] = (attended * gate_ref[mine, head : head + 1]).astype(jnp.bfloat16)


def attend(queries, gates, table, half):
    rows, width = queries.shape
    rows = rows // 2
    holders, slots, both = table.shape
    return pl.pallas_call(
        attend_kernel,
        grid=(1,),
        in_specs=[
            pl.BlockSpec((rows, width), lambda i: (half, 0)),
            pl.BlockSpec((rows, gates.shape[1]), lambda i: (half, 0)),
            pl.BlockSpec((holders, slots // 2, both), lambda i: (0, half, 0)),
        ],
        out_specs=pl.BlockSpec((rows, width), lambda i: (0, 0)),
        out_shape=jax.ShapeDtypeStruct((rows, width), jnp.bfloat16),
        name="attend",
    )(queries, gates, table)


def add_products_kernel(weight_ref, base_ref, *refs):
    out_ref = refs[-1]
    total = base_ref[...]
    for k, piece_ref in enumerate(refs[:-1]):
        total = total + jnp.dot(piece_ref[...], weight_ref[k], preferred_element_type=jnp.float32)
    out_ref[...] = total


def add_products(base, half, pieces, weights):
    rows, narrow = pieces[0].shape
    width = base.shape[1]
    steps = rows // OUT_ROWS
    return pl.pallas_call(
        add_products_kernel,
        grid=(steps,),
        in_specs=[
            pl.BlockSpec((len(pieces), narrow, width), lambda i: (0, 0, 0)),
            pl.BlockSpec((OUT_ROWS, width), lambda i: (half * steps + i, 0)),
        ]
        + [pl.BlockSpec((OUT_ROWS, narrow), lambda i: (i, 0))] * len(pieces),
        out_specs=pl.BlockSpec((OUT_ROWS, width), lambda i: (i, 0)),
        out_shape=jax.ShapeDtypeStruct((rows, width), jnp.float32),
        name="add_products",
    )(weights, base, *pieces)


def finish_kernel(weight_ref, low_base, low_piece, high_base, high_piece, out_ref):
    step = pl.program_id(0)
    half = pl.num_programs(0) // 2
    for place, base_ref, piece_ref in ((0, low_base, low_piece), (1, high_base, high_piece)):

        @pl.when(step // half == place)
        def _():
            total = base_ref[...] + jnp.dot(
                piece_ref[...], weight_ref[0], preferred_element_type=jnp.float32
            )
            out_ref[...] = total.astype(out_ref.dtype)


def finish(weights, low_base, low_piece, high_base, high_piece):
    rows, width = low_base.shape
    narrow = low_piece.shape[1]
    steps = rows // OUT_ROWS
    last = weights.shape[0] - 1

    def low(i):
        return jnp.minimum(i, steps - 1), 0

    def high(i):
        return jnp.maximum(i - steps, 0), 0

    return pl.pallas_call(
        finish_kernel,
        grid=(2 * steps,),
        in_specs=[
            pl.BlockSpec((1, narrow, width), lambda i: (last, 0, 0)),
            pl.BlockSpec((OUT_ROWS, width), low),
            pl.BlockSpec((OUT_ROWS, narrow), low),
            pl.BlockSpec((OUT_ROWS, width), high),
            pl.BlockSpec((OUT_ROWS, narrow), high),
        ],
        out_specs=pl.BlockSpec((OUT_ROWS, width), lambda i: (i, 0)),
        out_shape=jax.ShapeDtypeStruct((2 * rows, width), jnp.bfloat16),
        name="finish",
    )(weights, low_base, low_piece, high_base, high_piece)


def per_device(
    tokens,
    norm_gain,
    pool_weight,
    pool_scale,
    query_weight,
    gate_weight,
    key_weight,
    value_weight,
    out_weight,
    passage_gain,
    passage_store,
    passage_ids,
):
    head_index = lax.axis_index("tp")
    tp_count = lax.axis_size("tp")
    tok_rows, width_local = tokens.shape
    full_width = width_local * tp_count
    local_heads = query_weight.shape[1] // HD
    st_count = lax.axis_size("st")
    passages = passage_store.shape[0]
    shares = PLEN // st_count
    spread = spread_store(
        passage_ids.T, passage_store, passage_gain, key_weight, value_weight, st_count
    )
    held = lax.all_to_all(spread, "st", split_axis=0, concat_axis=0, tiled=True)
    width_both = key_weight.shape[1] + value_weight.shape[1]
    packed = select_rows(held, tok_rows // BLK, shares * passages, width_both)
    returned = lax.all_to_all(
        packed.reshape(st_count, -1, width_both), "st", split_axis=0, concat_axis=0, tiled=True
    )

    wide_tokens = tokens.astype(jnp.float32)
    square_sums = lax.psum(jnp.sum(wide_tokens * wide_tokens, axis=1), "tp")
    inverse = lax.rsqrt(square_sums / full_width + epsilon)
    gain_local = lax.dynamic_slice_in_dim(norm_gain, head_index * width_local, width_local)
    normed = (wide_tokens * inverse[:, None] * gain_local[None, :]).astype(jnp.bfloat16)
    up = [(i, (i + 1) % tp_count) for i in range(tp_count)]
    down = [(i, (i - 1) % tp_count) for i in range(tp_count)]
    half = tok_rows // 2
    turned = (head_index + jnp.array([0, tp_count - 1, 1, 2], dtype=jnp.int32)) % tp_count
    before = lax.ppermute(normed, "tp", up)
    after = lax.ppermute(normed, "tp", down)
    far_low = lax.ppermute(before[:half], "tp", up)
    far_high = lax.ppermute(after[half:], "tp", down)
    far = jnp.concatenate([far_low, far_high], axis=0)
    columns = jnp.concatenate([normed, before, after, far], axis=1)

    sequences = tok_rows // SEQ_LEN
    window = jnp.left_shift(jnp.int32(2), head_index)
    grouped = normed.astype(jnp.float32).reshape(sequences, SEQ_LEN, width_local)
    total = grouped
    for level in range(GROUPS):
        shift = 2**level
        moved = jnp.pad(total, ((0, 0), (shift, 0), (0, 0)))[:, :SEQ_LEN]
        total = jnp.where(level <= head_index, total + moved, total)
    position = jnp.arange(SEQ_LEN, dtype=jnp.int32)
    divisor = jnp.minimum(position + 1, window).astype(jnp.float32)
    pooled = (
        (total / divisor[None, :, None] - grouped)
        .astype(jnp.bfloat16)
        .reshape(tok_rows, width_local)
    )
    base = (
        jnp.dot(pooled, pool_weight[0], preferred_element_type=jnp.float32) * pool_scale[None, :]
    )

    def turn(weight):
        pieces = weight.reshape(tp_count, weight.shape[0] // tp_count, weight.shape[1])
        return jnp.take(pieces, turned, axis=0, mode="clip")

    gate_columns = lax.dynamic_slice_in_dim(
        gate_weight, head_index * local_heads, local_heads, axis=1
    )
    query_sum = jnp.dot(
        columns, turn(query_weight).reshape(query_weight.shape), preferred_element_type=jnp.float32
    )
    gate_sum = jnp.dot(
        columns, turn(gate_columns).reshape(gate_columns.shape), preferred_element_type=jnp.float32
    )
    queries = query_sum.astype(jnp.bfloat16)
    gating = jax.nn.sigmoid(gate_sum)

    weights = turn(out_weight)
    queries, gating, base, weights = lax.optimization_barrier((queries, gating, base, weights))

    low = attend(queries, gating, returned, 0)
    low_before = lax.ppermute(low, "tp", up)
    low_after = lax.ppermute(low, "tp", down)
    high = attend(queries, gating, returned, 1)
    high_before = lax.ppermute(high, "tp", up)
    high_after = lax.ppermute(high, "tp", down)
    low_far = lax.ppermute(low_before, "tp", up)
    high_far = lax.ppermute(high_after, "tp", down)
    low_base = add_products(base, 0, (low, low_before, low_after), weights)
    high_base = add_products(base, 1, (high, high_before, high_after), weights)
    return finish(weights, low_base, low_far, high_base, high_far)


def solution(mesh):
    in_specs = (
        P(("grp", "st"), "tp"),
        P(),
        P("tp", None, None),
        P("tp"),
        P(None, "tp"),
        P(),
        P(None, "tp"),
        P(None, "tp"),
        P(None, "tp"),
        P(),
        P(("grp", "st"), None, None),
        P(("grp", "st"), None),
    )
    out_specs = P(("grp", "st"), "tp")
    return jax.shard_map(per_device, mesh=mesh, in_specs=in_specs, out_specs=out_specs, check_vma=False)
```

```python
import jax
import jax.numpy as jnp
from jax import lax
from jax.experimental import pallas as pl
from jax.experimental.pallas import tpu as pltpu
from jax.sharding import PartitionSpec as P

HD = 128
GROUPS = 4
SEQ_LEN = 256
BLK = 128
NPB = 4
PLEN = 64

epsilon = 1e-06
LANES = 128
TILE = 8
SHARE_ROWS = 16
SELECT_READERS = 8
whole = pl.BlockSpec(memory_space=pltpu.VMEM)


def spread_kernel(ids_ref, store_ref, gain_ref, key_ref, value_ref, out_ref, order_ref, both_ref):
    step = pl.program_id(0)
    passages, span, width = store_ref.shape
    rows = passages * span
    holders, length, _ = out_ref.shape
    groups = holders // span
    half = key_ref.shape[1]
    chunks = 2 * half // LANES
    body = (length - TILE) // chunks

    @pl.when(step == 0)
    def _():
        both_ref[:, :half] = key_ref[...]
        both_ref[:, half:] = value_ref[...]
        spot = lax.broadcasted_iota(jnp.int32, (rows, rows), 0)
        holder = jnp.floor((spot.astype(jnp.float32) + 0.5) * (1.0 / passages)).astype(jnp.int32)
        wanted = (spot - holder * passages) * span + holder
        other = lax.broadcasted_iota(jnp.int32, (rows, rows), 1)
        order_ref[...] = jnp.where(wanted == other, 1.0, 0.0).astype(jnp.bfloat16)
        ids = ids_ref[...]
        ids = jnp.concatenate([ids] * (TILE // NPB), axis=0)
        share = lax.broadcasted_iota(jnp.int32, ids.shape, 0) // NPB
        owner = lax.div(ids, jnp.int32(passages))
        inside = ids - owner * passages + share * passages
        spare = jnp.zeros((TILE, LANES - 2 * ids.shape[1]), jnp.int32)
        tile = jnp.concatenate([owner, inside, spare], axis=1)
        tile = tile.astype(jnp.float32).astype(jnp.bfloat16)
        out_ref[:, length - TILE :, :] = jnp.broadcast_to(tile, (holders, TILE, LANES))

    wide = store_ref[...].astype(jnp.float32).reshape(rows, width)
    inverse = lax.rsqrt(jnp.mean(wide * wide, axis=-1, keepdims=True) + epsilon)
    scaled = (wide * gain_ref[...]).astype(jnp.bfloat16)
    first = pl.multiple_of((step % groups) * span, span)
    offset = (step // groups) * passages
    product = jnp.dot(scaled, both_ref[...], preferred_element_type=jnp.float32)
    product = (product * inverse).astype(jnp.bfloat16)
    turned = jnp.dot(order_ref[...], product, preferred_element_type=jnp.float32)
    turned = turned.reshape(span, passages, chunks * LANES).astype(jnp.bfloat16)
    for chunk in range(chunks):
        start = pl.multiple_of(chunk * body + offset, TILE)
        out_ref[pl.ds(first, span), pl.ds(start, passages), :] = turned[
            :, :, chunk * LANES : (chunk + 1) * LANES
        ]


def spread_store(ids, store, gain, key_weight, value_weight, holders):
    passages, length, width = store.shape
    head_width = key_weight.shape[1]
    rows = passages * SHARE_ROWS
    per_holder = passages * length // holders * (2 * head_width // LANES) + TILE
    return pl.pallas_call(
        spread_kernel,
        grid=(length // SHARE_ROWS,),
        in_specs=[
            pl.BlockSpec(ids.shape, lambda i: (0, 0)),
            pl.BlockSpec((passages, SHARE_ROWS, width), lambda i: (0, i, 0)),
            pl.BlockSpec((1, width), lambda i: (0, 0)),
            pl.BlockSpec((width, head_width), lambda i: (0, 0)),
            pl.BlockSpec((width, head_width), lambda i: (0, 0)),
        ],
        out_specs=pl.BlockSpec((holders, per_holder, LANES), lambda i: (0, 0, 0)),
        out_shape=jax.ShapeDtypeStruct((holders, per_holder, LANES), jnp.bfloat16),
        scratch_shapes=[
            pltpu.VMEM((rows, rows), jnp.bfloat16),
            pltpu.VMEM((width, 2 * head_width), jnp.bfloat16),
        ],
        name="spread_store",
    )(ids, store, gain.reshape(1, width), key_weight, value_weight)


def select_kernel(blocks, held_ref, out_ref, table_ref):
    step = pl.program_id(0)
    owners = held_ref.shape[0]
    chunks = table_ref.shape[1] // LANES
    body = table_ref.shape[0] // owners

    @pl.when(step == 0)
    def _():
        for owner in range(owners):
            for chunk in range(chunks):
                table_ref[
                    owner * body : (owner + 1) * body, chunk * LANES : (chunk + 1) * LANES
                ] = held_ref[owner, chunk * body : (chunk + 1) * body, :]

    spot = lax.broadcasted_iota(jnp.int32, (TILE, table_ref.shape[0]), 1).astype(jnp.float32)
    chosen = []
    for reader in range(SELECT_READERS):
        tile = held_ref[step * SELECT_READERS + reader, chunks * body :, :].astype(jnp.float32)
        for block in range(blocks):
            wanted = tile[:, block : block + 1] * float(body)
            wanted = wanted + tile[:, blocks + block : blocks + block + 1]
            chosen.append(jnp.where(spot == wanted, 1.0, 0.0))
    chosen = jnp.concatenate(chosen, axis=0).astype(jnp.bfloat16)
    out_ref[...] = jnp.dot(chosen, table_ref[...], preferred_element_type=jnp.float32).astype(
        jnp.bfloat16
    )


def select_rows(held, blocks, body, width):
    owners = held.shape[0]
    step_rows = SELECT_READERS * blocks * TILE
    return pl.pallas_call(
        lambda *refs: select_kernel(blocks, *refs),
        grid=(owners // SELECT_READERS,),
        in_specs=[whole],
        out_specs=pl.BlockSpec((step_rows, width), lambda i: (i, 0)),
        out_shape=jax.ShapeDtypeStruct((owners * blocks * TILE, width), jnp.bfloat16),
        scratch_shapes=[pltpu.VMEM((owners * body, width), jnp.bfloat16)],
        name="select_rows",
    )(held)


def attend_kernel(query_ref, gate_ref, table_ref, out_ref):
    holders, _, both = table_ref.shape
    width = query_ref.shape[1]
    rows = out_ref.shape[0]
    for block in range(rows // BLK):
        mine = slice(block * BLK, (block + 1) * BLK)
        table = table_ref[:, block * TILE : (block + 1) * TILE, :].astype(jnp.float32)
        table = table.reshape(holders * TILE, both).astype(jnp.bfloat16)
        for head in range(width // HD):
            cols = slice(head * HD, (head + 1) * HD)
            late = slice(width + head * HD, width + (head + 1) * HD)
            scores = lax.dot_general(
                query_ref[mine, cols],
                table[:, cols],
                (((1,), (1,)), ((), ())),
                preferred_element_type=jnp.float32,
            ) * HD ** (-0.5)
            weights = jnp.exp(scores - jnp.max(scores, axis=-1, keepdims=True))
            total = jnp.sum(weights, axis=-1, keepdims=True)
            probabilities = (weights * (1.0 / total)).astype(jnp.bfloat16)
            attended = jnp.dot(probabilities, table[:, late], preferred_element_type=jnp.float32)
            out_ref[mine, cols] = (attended * gate_ref[mine, head : head + 1]).astype(jnp.bfloat16)


def attend(queries, gates, table, half):
    rows, width = queries.shape
    rows = rows // 2
    holders, slots, both = table.shape
    return pl.pallas_call(
        attend_kernel,
        grid=(1,),
        in_specs=[
            pl.BlockSpec((rows, width), lambda i: (half, 0)),
            pl.BlockSpec((rows, gates.shape[1]), lambda i: (half, 0)),
            pl.BlockSpec((holders, slots // 2, both), lambda i: (0, half, 0)),
        ],
        out_specs=pl.BlockSpec((rows, width), lambda i: (0, 0)),
        out_shape=jax.ShapeDtypeStruct((rows, width), jnp.bfloat16),
        name="attend",
    )(queries, gates, table)


def per_device(
    tokens,
    norm_gain,
    pool_weight,
    pool_scale,
    query_weight,
    gate_weight,
    key_weight,
    value_weight,
    out_weight,
    passage_gain,
    passage_store,
    passage_ids,
):
    head_index = lax.axis_index("tp")
    tp_count = lax.axis_size("tp")
    tok_rows, width_local = tokens.shape
    full_width = width_local * tp_count
    local_heads = query_weight.shape[1] // HD
    st_count = lax.axis_size("st")
    passages = passage_store.shape[0]
    shares = PLEN // st_count
    spread = spread_store(
        passage_ids.T, passage_store, passage_gain, key_weight, value_weight, st_count
    )
    held = lax.all_to_all(spread, "st", split_axis=0, concat_axis=0, tiled=True)
    width_both = key_weight.shape[1] + value_weight.shape[1]
    packed = select_rows(held, tok_rows // BLK, shares * passages, width_both)
    returned = lax.all_to_all(
        packed.reshape(st_count, -1, width_both), "st", split_axis=0, concat_axis=0, tiled=True
    )

    wide_tokens = tokens.astype(jnp.float32)
    square_sums = lax.psum(jnp.sum(wide_tokens * wide_tokens, axis=1), "tp")
    inverse = lax.rsqrt(square_sums / full_width + epsilon)
    gain_local = lax.dynamic_slice_in_dim(norm_gain, head_index * width_local, width_local)
    normed = (wide_tokens * inverse[:, None] * gain_local[None, :]).astype(jnp.bfloat16)
    up = [(i, (i + 1) % tp_count) for i in range(tp_count)]
    down = [(i, (i - 1) % tp_count) for i in range(tp_count)]
    half = tok_rows // 2
    turned = (head_index + jnp.array([0, tp_count - 1, 1, 2], dtype=jnp.int32)) % tp_count
    before = lax.ppermute(normed, "tp", up)
    after = lax.ppermute(normed, "tp", down)
    far_low = lax.ppermute(before[:half], "tp", up)
    far_high = lax.ppermute(after[half:], "tp", down)
    far = jnp.concatenate([far_low, far_high], axis=0)
    columns = jnp.concatenate([normed, before, after, far], axis=1)

    sequences = tok_rows // SEQ_LEN
    window = jnp.left_shift(jnp.int32(2), head_index)
    grouped = normed.astype(jnp.float32).reshape(sequences, SEQ_LEN, width_local)
    total = grouped
    for level in range(GROUPS):
        shift = 2**level
        moved = jnp.pad(total, ((0, 0), (shift, 0), (0, 0)))[:, :SEQ_LEN]
        total = jnp.where(level <= head_index, total + moved, total)
    position = jnp.arange(SEQ_LEN, dtype=jnp.int32)
    divisor = jnp.minimum(position + 1, window).astype(jnp.float32)
    pooled = (
        (total / divisor[None, :, None] - grouped)
        .astype(jnp.bfloat16)
        .reshape(tok_rows, width_local)
    )
    base = (
        jnp.dot(pooled, pool_weight[0], preferred_element_type=jnp.float32) * pool_scale[None, :]
    )

    def turn(weight):
        pieces = weight.reshape(tp_count, weight.shape[0] // tp_count, weight.shape[1])
        return jnp.take(pieces, turned, axis=0, mode="clip")

    gate_columns = lax.dynamic_slice_in_dim(
        gate_weight, head_index * local_heads, local_heads, axis=1
    )
    query_sum = jnp.dot(
        columns, turn(query_weight).reshape(query_weight.shape), preferred_element_type=jnp.float32
    )
    gate_sum = jnp.dot(
        columns, turn(gate_columns).reshape(gate_columns.shape), preferred_element_type=jnp.float32
    )
    queries = query_sum.astype(jnp.bfloat16)
    gating = jax.nn.sigmoid(gate_sum)

    weights = turn(out_weight)
    queries, gating, base, weights = lax.optimization_barrier((queries, gating, base, weights))

    low = attend(queries, gating, returned, 0)
    low_before = lax.ppermute(low, "tp", up)
    low_after = lax.ppermute(low, "tp", down)
    high = attend(queries, gating, returned, 1)
    high_before = lax.ppermute(high, "tp", up)
    high_after = lax.ppermute(high, "tp", down)
    low_far = lax.ppermute(low_before, "tp", up)
    high_far = lax.ppermute(high_after, "tp", down)
    near = weights[:3].reshape(-1, width_local)
    low_near = jnp.concatenate([low, low_before, low_after], axis=1)
    low_base = base[:half] + jnp.dot(low_near, near, preferred_element_type=jnp.float32)
    high_near = jnp.concatenate([high, high_before, high_after], axis=1)
    high_base = base[half:] + jnp.dot(high_near, near, preferred_element_type=jnp.float32)
    low_base, high_base = lax.optimization_barrier((low_base, high_base))
    far = jnp.concatenate([low_far, high_far], axis=0)
    base = jnp.concatenate([low_base, high_base], axis=0)
    return (base + jnp.dot(far, weights[3], preferred_element_type=jnp.float32)).astype(
        jnp.bfloat16
    )


def solution(mesh):
    in_specs = (
        P(("grp", "st"), "tp"),
        P(),
        P("tp", None, None),
        P("tp"),
        P(None, "tp"),
        P(),
        P(None, "tp"),
        P(None, "tp"),
        P(None, "tp"),
        P(),
        P(("grp", "st"), None, None),
        P(("grp", "st"), None),
    )
    out_specs = P(("grp", "st"), "tp")
    return jax.shard_map(per_device, mesh=mesh, in_specs=in_specs, out_specs=out_specs, check_vma=False)
```

```python
import jax
import jax.numpy as jnp
from jax import lax
from jax.experimental import pallas as pl
from jax.experimental.pallas import tpu as pltpu
from jax.sharding import PartitionSpec as P

HD = 128
GROUPS = 4
SEQ_LEN = 256
BLK = 128
NPB = 4
PLEN = 64

epsilon = 1e-06
LANES = 128
TILE = 8
SHARE_ROWS = 16
SELECT_READERS = 8
whole = pl.BlockSpec(memory_space=pltpu.VMEM)


def spread_kernel(ids_ref, store_ref, gain_ref, key_ref, value_ref, out_ref, order_ref, both_ref):
    step = pl.program_id(0)
    passages, span, width = store_ref.shape
    rows = passages * span
    holders, length, _ = out_ref.shape
    groups = holders // span
    half = key_ref.shape[1]
    chunks = 2 * half // LANES
    body = (length - TILE) // chunks

    @pl.when(step == 0)
    def _():
        both_ref[:, :half] = key_ref[...]
        both_ref[:, half:] = value_ref[...]
        spot = lax.broadcasted_iota(jnp.int32, (rows, rows), 0)
        holder = jnp.floor((spot.astype(jnp.float32) + 0.5) * (1.0 / passages)).astype(jnp.int32)
        wanted = (spot - holder * passages) * span + holder
        other = lax.broadcasted_iota(jnp.int32, (rows, rows), 1)
        order_ref[...] = jnp.where(wanted == other, 1.0, 0.0).astype(jnp.bfloat16)
        ids = ids_ref[...]
        ids = jnp.concatenate([ids] * (TILE // NPB), axis=0)
        owner = lax.div(ids, jnp.int32(passages))
        inside = ids - owner * passages
        spare = jnp.zeros((TILE, LANES - 2 * ids.shape[1]), jnp.int32)
        tile = jnp.concatenate([owner, inside, spare], axis=1)
        tile = tile.astype(jnp.float32).astype(jnp.bfloat16)
        out_ref[:, length - TILE :, :] = jnp.broadcast_to(tile, (holders, TILE, LANES))

    wide = store_ref[...].astype(jnp.float32).reshape(rows, width)
    inverse = lax.rsqrt(jnp.mean(wide * wide, axis=-1, keepdims=True) + epsilon)
    scaled = (wide * gain_ref[...]).astype(jnp.bfloat16)
    first = pl.multiple_of((step % groups) * span, span)
    offset = (step // groups) * passages
    product = jnp.dot(scaled, both_ref[...], preferred_element_type=jnp.float32)
    product = (product * inverse).astype(jnp.bfloat16)
    turned = jnp.dot(order_ref[...], product, preferred_element_type=jnp.float32)
    turned = turned.reshape(span, passages, chunks * LANES).astype(jnp.bfloat16)
    for chunk in range(chunks):
        start = pl.multiple_of(chunk * body + offset, TILE)
        out_ref[pl.ds(first, span), pl.ds(start, passages), :] = turned[
            :, :, chunk * LANES : (chunk + 1) * LANES
        ]


def spread_store(ids, store, gain, key_weight, value_weight, holders):
    passages, length, width = store.shape
    head_width = key_weight.shape[1]
    rows = passages * SHARE_ROWS
    per_holder = passages * length // holders * (2 * head_width // LANES) + TILE
    return pl.pallas_call(
        spread_kernel,
        grid=(length // SHARE_ROWS,),
        in_specs=[
            pl.BlockSpec(ids.shape, lambda i: (0, 0)),
            pl.BlockSpec((passages, SHARE_ROWS, width), lambda i: (0, i, 0)),
            pl.BlockSpec((1, width), lambda i: (0, 0)),
            pl.BlockSpec((width, head_width), lambda i: (0, 0)),
            pl.BlockSpec((width, head_width), lambda i: (0, 0)),
        ],
        out_specs=pl.BlockSpec((holders, per_holder, LANES), lambda i: (0, 0, 0)),
        out_shape=jax.ShapeDtypeStruct((holders, per_holder, LANES), jnp.bfloat16),
        scratch_shapes=[
            pltpu.VMEM((rows, rows), jnp.bfloat16),
            pltpu.VMEM((width, 2 * head_width), jnp.bfloat16),
        ],
        name="spread_store",
    )(ids, store, gain.reshape(1, width), key_weight, value_weight)


def select_kernel(blocks, shares, held_ref, out_ref, table_ref):
    step = pl.program_id(0)
    owners, length, _ = held_ref.shape
    passages = table_ref.shape[0] // owners
    width = table_ref.shape[1]
    chunks = width // shares // LANES

    @pl.when(step == 0)
    def _():
        for owner in range(owners):
            rows = slice(owner * passages, (owner + 1) * passages)
            for share in range(shares):
                for chunk in range(chunks):
                    source = (chunk * shares + share) * passages
                    lane = (share * chunks + chunk) * LANES
                    table_ref[rows, lane : lane + LANES] = held_ref[
                        owner, source : source + passages, :
                    ]

    spot = lax.broadcasted_iota(jnp.int32, (TILE, table_ref.shape[0]), 1).astype(jnp.float32)
    early = lax.broadcasted_iota(jnp.int32, (TILE, 1), 0) < NPB
    chosen = []
    for reader in range(SELECT_READERS):
        tile = held_ref[step * SELECT_READERS + reader, length - TILE :, :].astype(jnp.float32)
        wanted = tile[:, :blocks] * float(passages) + tile[:, blocks : 2 * blocks]
        for pair in range(0, blocks, 2):
            mine = jnp.where(early, wanted[:, pair : pair + 1], wanted[:, pair + 1 : pair + 2])
            chosen.append(jnp.where(spot == mine, 1.0, 0.0))
    chosen = jnp.concatenate(chosen, axis=0).astype(jnp.bfloat16)
    out_ref[...] = jnp.dot(chosen, table_ref[...], preferred_element_type=jnp.float32).astype(
        jnp.bfloat16
    )


def select_rows(held, blocks, passages, shares, width):
    owners = held.shape[0]
    step_rows = SELECT_READERS * blocks * NPB
    return pl.pallas_call(
        lambda *refs: select_kernel(blocks, shares, *refs),
        grid=(owners // SELECT_READERS,),
        in_specs=[whole],
        out_specs=pl.BlockSpec((step_rows, shares * width), lambda i: (i, 0)),
        out_shape=jax.ShapeDtypeStruct((owners * blocks * NPB, shares * width), jnp.bfloat16),
        scratch_shapes=[pltpu.VMEM((owners * passages, shares * width), jnp.bfloat16)],
        name="select_rows",
    )(held)


def attend_kernel(query_ref, gate_ref, table_ref, out_ref):
    holders, slots, _ = table_ref.shape
    width = query_ref.shape[1]
    both = 2 * width
    early = lax.broadcasted_iota(jnp.int32, (holders, TILE, both), 1) < NPB
    for pair in range(slots // TILE):
        here = slice(pair * TILE, (pair + 1) * TILE)
        first = table_ref[:, here, :both].astype(jnp.float32)
        second = table_ref[:, here, both:].astype(jnp.float32)
        tables = (
            jnp.where(early, first, pltpu.roll(second, NPB, 1)),
            jnp.where(early, pltpu.roll(first, NPB, 1), second),
        )
        for place, table in enumerate(tables):
            table = table.reshape(holders * TILE, both).astype(jnp.bfloat16)
            block = 2 * pair + place
            mine = slice(block * BLK, (block + 1) * BLK)
            for head in range(width // HD):
                cols = slice(head * HD, (head + 1) * HD)
                late = slice(width + head * HD, width + (head + 1) * HD)
                scores = lax.dot_general(
                    query_ref[mine, cols],
                    table[:, cols],
                    (((1,), (1,)), ((), ())),
                    preferred_element_type=jnp.float32,
                ) * HD ** (-0.5)
                weights = jnp.exp(scores - jnp.max(scores, axis=-1, keepdims=True))
                total = jnp.sum(weights, axis=-1, keepdims=True)
                probabilities = (weights * (1.0 / total)).astype(jnp.bfloat16)
                attended = jnp.dot(
                    probabilities, table[:, late], preferred_element_type=jnp.float32
                )
                out_ref[mine, cols] = (attended * gate_ref[mine, head : head + 1]).astype(
                    jnp.bfloat16
                )


def attend(queries, gates, table, half):
    rows, width = queries.shape
    rows = rows // 2
    holders, slots, both = table.shape
    return pl.pallas_call(
        attend_kernel,
        grid=(1,),
        in_specs=[
            pl.BlockSpec((rows, width), lambda i: (half, 0)),
            pl.BlockSpec((rows, gates.shape[1]), lambda i: (half, 0)),
            pl.BlockSpec((holders, slots // 2, both), lambda i: (0, half, 0)),
        ],
        out_specs=pl.BlockSpec((rows, width), lambda i: (0, 0)),
        out_shape=jax.ShapeDtypeStruct((rows, width), jnp.bfloat16),
        name="attend",
    )(queries, gates, table)


def per_device(
    tokens,
    norm_gain,
    pool_weight,
    pool_scale,
    query_weight,
    gate_weight,
    key_weight,
    value_weight,
    out_weight,
    passage_gain,
    passage_store,
    passage_ids,
):
    head_index = lax.axis_index("tp")
    tp_count = lax.axis_size("tp")
    tok_rows, width_local = tokens.shape
    full_width = width_local * tp_count
    local_heads = query_weight.shape[1] // HD
    st_count = lax.axis_size("st")
    passages = passage_store.shape[0]
    shares = PLEN // st_count
    spread = spread_store(
        passage_ids.T, passage_store, passage_gain, key_weight, value_weight, st_count
    )
    held = lax.all_to_all(spread, "st", split_axis=0, concat_axis=0, tiled=True)
    width_both = key_weight.shape[1] + value_weight.shape[1]
    packed = select_rows(held, tok_rows // BLK, passages, shares, width_both)
    returned = lax.all_to_all(
        packed.reshape(st_count, -1, shares * width_both),
        "st",
        split_axis=0,
        concat_axis=0,
        tiled=True,
    )

    wide_tokens = tokens.astype(jnp.float32)
    square_sums = lax.psum(jnp.sum(wide_tokens * wide_tokens, axis=1), "tp")
    inverse = lax.rsqrt(square_sums / full_width + epsilon)
    gain_local = lax.dynamic_slice_in_dim(norm_gain, head_index * width_local, width_local)
    normed = (wide_tokens * inverse[:, None] * gain_local[None, :]).astype(jnp.bfloat16)
    up = [(i, (i + 1) % tp_count) for i in range(tp_count)]
    down = [(i, (i - 1) % tp_count) for i in range(tp_count)]
    across = [(i, (i + 2) % tp_count) for i in range(tp_count)]
    half = tok_rows // 2
    turned = (head_index + jnp.array([0, tp_count - 1, 1, 2], dtype=jnp.int32)) % tp_count
    before = lax.ppermute(normed, "tp", up)
    after = lax.ppermute(normed, "tp", down)
    far = lax.ppermute(normed, "tp", across)
    columns = jnp.concatenate([normed, before, after, far], axis=1)

    sequences = tok_rows // SEQ_LEN
    window = jnp.left_shift(jnp.int32(2), head_index)
    grouped = normed.astype(jnp.float32).reshape(sequences, SEQ_LEN, width_local)
    total = grouped
    for level in range(GROUPS):
        shift = 2**level
        moved = jnp.pad(total, ((0, 0), (shift, 0), (0, 0)))[:, :SEQ_LEN]
        total = jnp.where(level <= head_index, total + moved, total)
    position = jnp.arange(SEQ_LEN, dtype=jnp.int32)
    divisor = jnp.minimum(position + 1, window).astype(jnp.float32)
    pooled = (
        (total / divisor[None, :, None] - grouped)
        .astype(jnp.bfloat16)
        .reshape(tok_rows, width_local)
    )
    base = (
        jnp.dot(pooled, pool_weight[0], preferred_element_type=jnp.float32) * pool_scale[None, :]
    )

    def turn(weight):
        pieces = weight.reshape(tp_count, weight.shape[0] // tp_count, weight.shape[1])
        return jnp.take(pieces, turned, axis=0, mode="clip")

    gate_columns = lax.dynamic_slice_in_dim(
        gate_weight, head_index * local_heads, local_heads, axis=1
    )
    query_sum = jnp.dot(
        columns, turn(query_weight).reshape(query_weight.shape), preferred_element_type=jnp.float32
    )
    gate_sum = jnp.dot(
        columns, turn(gate_columns).reshape(gate_columns.shape), preferred_element_type=jnp.float32
    )
    queries = query_sum.astype(jnp.bfloat16)
    gating = jax.nn.sigmoid(gate_sum)

    weights = turn(out_weight)
    queries, gating, base, weights = lax.optimization_barrier((queries, gating, base, weights))

    low = attend(queries, gating, returned, 0)
    low_before = lax.ppermute(low, "tp", up)
    low_after = lax.ppermute(low, "tp", down)
    high = attend(queries, gating, returned, 1)
    high_before = lax.ppermute(high, "tp", up)
    high_after = lax.ppermute(high, "tp", down)
    low_far = lax.ppermute(low, "tp", across)
    high_far = lax.ppermute(high, "tp", across)
    near = weights[:3].reshape(-1, width_local)
    low_near = jnp.concatenate([low, low_before, low_after], axis=1)
    low_base = base[:half] + jnp.dot(low_near, near, preferred_element_type=jnp.float32)
    high_near = jnp.concatenate([high, high_before, high_after], axis=1)
    high_base = base[half:] + jnp.dot(high_near, near, preferred_element_type=jnp.float32)
    low_base, high_base = lax.optimization_barrier((low_base, high_base))
    far = jnp.concatenate([low_far, high_far], axis=0)
    base = jnp.concatenate([low_base, high_base], axis=0)
    return (base + jnp.dot(far, weights[3], preferred_element_type=jnp.float32)).astype(
        jnp.bfloat16
    )


def solution(mesh):
    in_specs = (
        P(("grp", "st"), "tp"),
        P(),
        P("tp", None, None),
        P("tp"),
        P(None, "tp"),
        P(),
        P(None, "tp"),
        P(None, "tp"),
        P(None, "tp"),
        P(),
        P(("grp", "st"), None, None),
        P(("grp", "st"), None),
    )
    out_specs = P(("grp", "st"), "tp")
    return jax.shard_map(per_device, mesh=mesh, in_specs=in_specs, out_specs=out_specs, check_vma=False)
```

```python
import jax
import jax.numpy as jnp
from jax import lax
from jax.experimental import pallas as pl
from jax.experimental.pallas import tpu as pltpu
from jax.sharding import PartitionSpec as P

HD = 128
GROUPS = 4
SEQ_LEN = 256
BLK = 128
NPB = 4
PLEN = 64

epsilon = 1e-06
LANES = 128
TILE = 8
SHARE_ROWS = 16
SELECT_READERS = 16
whole = pl.BlockSpec(memory_space=pltpu.VMEM)


def spread_kernel(ids_ref, store_ref, gain_ref, key_ref, value_ref, out_ref, order_ref, both_ref):
    group, share = pl.program_id(0), pl.program_id(1)
    passages, span, width = store_ref.shape
    rows = passages * span
    length = out_ref.shape[1]
    half = key_ref.shape[1]
    chunks = 2 * half // LANES
    body = (length - TILE) // chunks

    @pl.when((group == 0) & (share == 0))
    def _():
        both_ref[:, :half] = key_ref[...]
        both_ref[:, half:] = value_ref[...]
        spot = lax.broadcasted_iota(jnp.int32, (rows, rows), 0)
        holder = jnp.floor((spot.astype(jnp.float32) + 0.5) * (1.0 / passages)).astype(jnp.int32)
        wanted = (spot - holder * passages) * span + holder
        other = lax.broadcasted_iota(jnp.int32, (rows, rows), 1)
        order_ref[...] = jnp.where(wanted == other, 1.0, 0.0).astype(jnp.bfloat16)

    @pl.when(share == 0)
    def _():
        ids = ids_ref[...]
        ids = jnp.concatenate([ids] * (TILE // NPB), axis=0)
        owner = lax.div(ids, jnp.int32(passages))
        inside = ids - owner * passages
        spare = jnp.zeros((TILE, LANES - 2 * ids.shape[1]), jnp.int32)
        tile = jnp.concatenate([owner, inside, spare], axis=1)
        tile = tile.astype(jnp.float32).astype(jnp.bfloat16)
        out_ref[:, length - TILE :, :] = jnp.broadcast_to(tile, (span, TILE, LANES))

    wide = store_ref[...].astype(jnp.float32).reshape(rows, width)
    inverse = lax.rsqrt(jnp.mean(wide * wide, axis=-1, keepdims=True) + epsilon)
    scaled = (wide * gain_ref[...]).astype(jnp.bfloat16)
    product = jnp.dot(scaled, both_ref[...], preferred_element_type=jnp.float32)
    product = (product * inverse).astype(jnp.bfloat16)
    turned = jnp.dot(order_ref[...], product, preferred_element_type=jnp.float32)
    turned = turned.reshape(span, passages, chunks * LANES).astype(jnp.bfloat16)
    for chunk in range(chunks):
        start = pl.multiple_of(chunk * body + share * passages, TILE)
        out_ref[:, pl.ds(start, passages), :] = turned[
            :, :, chunk * LANES : (chunk + 1) * LANES
        ]


def spread_store(ids, store, gain, key_weight, value_weight, holders):
    passages, length, width = store.shape
    head_width = key_weight.shape[1]
    rows = passages * SHARE_ROWS
    per_holder = passages * length // holders * (2 * head_width // LANES) + TILE
    groups = holders // SHARE_ROWS
    return pl.pallas_call(
        spread_kernel,
        grid=(groups, length // holders),
        in_specs=[
            pl.BlockSpec(ids.shape, lambda g, i: (0, 0)),
            pl.BlockSpec((passages, SHARE_ROWS, width), lambda g, i: (0, i * groups + g, 0)),
            pl.BlockSpec((1, width), lambda g, i: (0, 0)),
            pl.BlockSpec((width, head_width), lambda g, i: (0, 0)),
            pl.BlockSpec((width, head_width), lambda g, i: (0, 0)),
        ],
        out_specs=pl.BlockSpec((SHARE_ROWS, per_holder, LANES), lambda g, i: (g, 0, 0)),
        out_shape=jax.ShapeDtypeStruct((holders, per_holder, LANES), jnp.bfloat16),
        scratch_shapes=[
            pltpu.VMEM((rows, rows), jnp.bfloat16),
            pltpu.VMEM((width, 2 * head_width), jnp.bfloat16),
        ],
        name="spread_store",
    )(ids, store, gain.reshape(1, width), key_weight, value_weight)


def select_kernel(blocks, shares, held_ref, out_ref, table_ref):
    step = pl.program_id(0)
    owners, length, _ = held_ref.shape
    passages = table_ref.shape[0] // owners
    width = table_ref.shape[1]
    chunks = width // shares // LANES

    @pl.when(step == 0)
    def _():
        for owner in range(owners):
            rows = slice(owner * passages, (owner + 1) * passages)
            for share in range(shares):
                for chunk in range(chunks):
                    source = (chunk * shares + share) * passages
                    lane = (share * chunks + chunk) * LANES
                    table_ref[rows, lane : lane + LANES] = held_ref[
                        owner, source : source + passages, :
                    ]

    spot = lax.broadcasted_iota(jnp.int32, (TILE, table_ref.shape[0]), 1).astype(jnp.float32)
    early = lax.broadcasted_iota(jnp.int32, (TILE, 1), 0) < NPB
    chosen = []
    for reader in range(SELECT_READERS):
        tile = held_ref[step * SELECT_READERS + reader, length - TILE :, :].astype(jnp.float32)
        wanted = tile[:, :blocks] * float(passages) + tile[:, blocks : 2 * blocks]
        for pair in range(0, blocks, 2):
            mine = jnp.where(early, wanted[:, pair : pair + 1], wanted[:, pair + 1 : pair + 2])
            chosen.append(jnp.where(spot == mine, 1.0, 0.0))
    chosen = jnp.concatenate(chosen, axis=0).astype(jnp.bfloat16)
    out_ref[...] = jnp.dot(chosen, table_ref[...], preferred_element_type=jnp.float32).astype(
        jnp.bfloat16
    )


def select_rows(held, blocks, passages, shares, width):
    owners = held.shape[0]
    step_rows = SELECT_READERS * blocks * NPB
    return pl.pallas_call(
        lambda *refs: select_kernel(blocks, shares, *refs),
        grid=(owners // SELECT_READERS,),
        in_specs=[whole],
        out_specs=pl.BlockSpec((step_rows, shares * width), lambda i: (i, 0)),
        out_shape=jax.ShapeDtypeStruct((owners * blocks * NPB, shares * width), jnp.bfloat16),
        scratch_shapes=[pltpu.VMEM((owners * passages, shares * width), jnp.bfloat16)],
        name="select_rows",
    )(held)


def attend_kernel(query_ref, gate_ref, table_ref, out_ref, keys_ref, scores_ref):
    holders, slots, _ = table_ref.shape
    rows, width = query_ref.shape
    both = 2 * width
    heads = width // HD
    early = lax.broadcasted_iota(jnp.int32, (holders, TILE, both), 1) < NPB
    for pair in range(slots // TILE):
        here = slice(pair * TILE, (pair + 1) * TILE)
        first = table_ref[:, here, :both].astype(jnp.float32)
        second = table_ref[:, here, both:].astype(jnp.float32)
        tables = (
            jnp.where(early, first, pltpu.roll(second, NPB, 1)),
            jnp.where(early, pltpu.roll(first, NPB, 1), second),
        )
        for place, table in enumerate(tables):
            keys_ref[2 * pair + place] = table.reshape(holders * TILE, both).astype(jnp.bfloat16)
    for head in range(heads):
        cols = slice(head * HD, (head + 1) * HD)
        for block in range(rows // BLK):
            mine = slice(block * BLK, (block + 1) * BLK)
            scores_ref[head, mine, :] = lax.dot_general(
                query_ref[mine, cols],
                keys_ref[block, :, cols],
                (((1,), (1,)), ((), ())),
                preferred_element_type=jnp.float32,
            ) * HD ** (-0.5)
    for head in range(heads):
        cols = slice(head * HD, (head + 1) * HD)
        late = slice(width + head * HD, width + (head + 1) * HD)
        scores = scores_ref[head]
        weights = jnp.exp(scores - jnp.max(scores, axis=-1, keepdims=True))
        total = jnp.sum(weights, axis=-1, keepdims=True)
        probabilities = (weights * (1.0 / total)).astype(jnp.bfloat16)
        for block in range(rows // BLK):
            mine = slice(block * BLK, (block + 1) * BLK)
            attended = jnp.dot(
                probabilities[mine, :], keys_ref[block, :, late], preferred_element_type=jnp.float32
            )
            out_ref[mine, cols] = (attended * gate_ref[mine, head : head + 1]).astype(jnp.bfloat16)


def attend(queries, gates, table, half):
    rows, width = queries.shape
    rows = rows // 2
    holders, slots, both = table.shape
    return pl.pallas_call(
        attend_kernel,
        grid=(1,),
        in_specs=[
            pl.BlockSpec((rows, width), lambda i: (half, 0)),
            pl.BlockSpec((rows, gates.shape[1]), lambda i: (half, 0)),
            pl.BlockSpec((holders, slots // 2, both), lambda i: (0, half, 0)),
        ],
        out_specs=pl.BlockSpec((rows, width), lambda i: (0, 0)),
        out_shape=jax.ShapeDtypeStruct((rows, width), jnp.bfloat16),
        scratch_shapes=[
            pltpu.VMEM((rows // BLK, holders * TILE, both // 2), jnp.bfloat16),
            pltpu.VMEM((width // HD, rows, holders * TILE), jnp.float32),
        ],
        name="attend",
    )(queries, gates, table)


def per_device(
    tokens,
    norm_gain,
    pool_weight,
    pool_scale,
    query_weight,
    gate_weight,
    key_weight,
    value_weight,
    out_weight,
    passage_gain,
    passage_store,
    passage_ids,
):
    head_index = lax.axis_index("tp")
    tp_count = lax.axis_size("tp")
    tok_rows, width_local = tokens.shape
    full_width = width_local * tp_count
    local_heads = query_weight.shape[1] // HD
    st_count = lax.axis_size("st")
    passages = passage_store.shape[0]
    shares = PLEN // st_count
    spread = spread_store(
        passage_ids.T, passage_store, passage_gain, key_weight, value_weight, st_count
    )
    held = lax.all_to_all(spread, "st", split_axis=0, concat_axis=0, tiled=True)
    width_both = key_weight.shape[1] + value_weight.shape[1]
    packed = select_rows(held, tok_rows // BLK, passages, shares, width_both)
    returned = lax.all_to_all(
        packed.reshape(st_count, -1, shares * width_both),
        "st",
        split_axis=0,
        concat_axis=0,
        tiled=True,
    )

    wide_tokens = tokens.astype(jnp.float32)
    square_sums = lax.psum(jnp.sum(wide_tokens * wide_tokens, axis=1), "tp")
    inverse = lax.rsqrt(square_sums / full_width + epsilon)
    gain_local = lax.dynamic_slice_in_dim(norm_gain, head_index * width_local, width_local)
    normed = (wide_tokens * inverse[:, None] * gain_local[None, :]).astype(jnp.bfloat16)
    up = [(i, (i + 1) % tp_count) for i in range(tp_count)]
    down = [(i, (i - 1) % tp_count) for i in range(tp_count)]
    across = [(i, (i + 2) % tp_count) for i in range(tp_count)]
    half = tok_rows // 2
    turned = (head_index + jnp.array([0, tp_count - 1, 1, 2], dtype=jnp.int32)) % tp_count
    before = lax.ppermute(normed, "tp", up)
    after = lax.ppermute(normed, "tp", down)
    far = lax.ppermute(normed, "tp", across)
    columns = jnp.concatenate([normed, before, after, far], axis=1)

    sequences = tok_rows // SEQ_LEN
    window = jnp.left_shift(jnp.int32(2), head_index)
    grouped = normed.astype(jnp.float32).reshape(sequences, SEQ_LEN, width_local)
    total = grouped
    for level in range(GROUPS):
        shift = 2**level
        moved = jnp.pad(total, ((0, 0), (shift, 0), (0, 0)))[:, :SEQ_LEN]
        total = jnp.where(level <= head_index, total + moved, total)
    position = jnp.arange(SEQ_LEN, dtype=jnp.int32)
    divisor = jnp.minimum(position + 1, window).astype(jnp.float32)
    pooled = (
        (total / divisor[None, :, None] - grouped)
        .astype(jnp.bfloat16)
        .reshape(tok_rows, width_local)
    )
    base = (
        jnp.dot(pooled, pool_weight[0], preferred_element_type=jnp.float32) * pool_scale[None, :]
    )

    def turn(weight):
        pieces = weight.reshape(tp_count, weight.shape[0] // tp_count, weight.shape[1])
        return jnp.take(pieces, turned, axis=0, mode="clip")

    gate_columns = lax.dynamic_slice_in_dim(
        gate_weight, head_index * local_heads, local_heads, axis=1
    )
    query_sum = jnp.dot(
        columns, turn(query_weight).reshape(query_weight.shape), preferred_element_type=jnp.float32
    )
    gate_sum = jnp.dot(
        columns, turn(gate_columns).reshape(gate_columns.shape), preferred_element_type=jnp.float32
    )
    queries = query_sum.astype(jnp.bfloat16)
    gating = jax.nn.sigmoid(gate_sum)

    weights = turn(out_weight)
    queries, gating, base, weights = lax.optimization_barrier((queries, gating, base, weights))

    low = attend(queries, gating, returned, 0)
    low_before = lax.ppermute(low, "tp", up)
    low_after = lax.ppermute(low, "tp", down)
    high = attend(queries, gating, returned, 1)
    high_before = lax.ppermute(high, "tp", up)
    high_after = lax.ppermute(high, "tp", down)
    low_far = lax.ppermute(low_before, "tp", up)
    high_far = lax.ppermute(high_after, "tp", down)
    near = weights[:3].reshape(-1, width_local)
    low_near = jnp.concatenate([low, low_before, low_after], axis=1)
    low_base = base[:half] + jnp.dot(low_near, near, preferred_element_type=jnp.float32)
    high_near = jnp.concatenate([high, high_before, high_after], axis=1)
    high_base = base[half:] + jnp.dot(high_near, near, preferred_element_type=jnp.float32)
    low_base, high_base = lax.optimization_barrier((low_base, high_base))
    far = jnp.concatenate([low_far, high_far], axis=0)
    base = jnp.concatenate([low_base, high_base], axis=0)
    return (base + jnp.dot(far, weights[3], preferred_element_type=jnp.float32)).astype(
        jnp.bfloat16
    )


def solution(mesh):
    in_specs = (
        P(("grp", "st"), "tp"),
        P(),
        P("tp", None, None),
        P("tp"),
        P(None, "tp"),
        P(),
        P(None, "tp"),
        P(None, "tp"),
        P(None, "tp"),
        P(),
        P(("grp", "st"), None, None),
        P(("grp", "st"), None),
    )
    out_specs = P(("grp", "st"), "tp")
    return jax.shard_map(per_device, mesh=mesh, in_specs=in_specs, out_specs=out_specs, check_vma=False)
```

```python
import jax
import jax.numpy as jnp
from jax import lax
from jax.experimental import pallas as pl
from jax.experimental.pallas import tpu as pltpu
from jax.sharding import PartitionSpec as P

HD = 128
GROUPS = 4
SEQ_LEN = 256
BLK = 128
NPB = 4
PLEN = 64

epsilon = 1e-06
LANES = 128
TILE = 8
SHARE_ROWS = 16
SELECT_READERS = 16
whole = pl.BlockSpec(memory_space=pltpu.VMEM)


def spread_kernel(ids_ref, store_ref, gain_ref, key_ref, value_ref, out_ref, order_ref, both_ref):
    group, share = pl.program_id(0), pl.program_id(1)
    passages, span, width = store_ref.shape
    rows = passages * span
    length = out_ref.shape[1]
    half = key_ref.shape[1]
    chunks = 2 * half // LANES
    body = (length - TILE) // chunks

    @pl.when((group == 0) & (share == 0))
    def _():
        both_ref[:, :half] = key_ref[...]
        both_ref[:, half:] = value_ref[...]
        spot = lax.broadcasted_iota(jnp.int32, (rows, rows), 0)
        holder = jnp.floor((spot.astype(jnp.float32) + 0.5) * (1.0 / passages)).astype(jnp.int32)
        wanted = (spot - holder * passages) * span + holder
        other = lax.broadcasted_iota(jnp.int32, (rows, rows), 1)
        order_ref[...] = jnp.where(wanted == other, 1.0, 0.0).astype(jnp.bfloat16)

    @pl.when(share == 0)
    def _():
        ids = ids_ref[...]
        ids = jnp.concatenate([ids] * (TILE // NPB), axis=0)
        owner = lax.div(ids, jnp.int32(passages))
        inside = ids - owner * passages
        spare = jnp.zeros((TILE, LANES - 2 * ids.shape[1]), jnp.int32)
        tile = jnp.concatenate([owner, inside, spare], axis=1)
        tile = tile.astype(jnp.float32).astype(jnp.bfloat16)
        out_ref[:, length - TILE :, :] = jnp.broadcast_to(tile, (span, TILE, LANES))

    wide = store_ref[...].astype(jnp.float32).reshape(rows, width)
    inverse = lax.rsqrt(jnp.mean(wide * wide, axis=-1, keepdims=True) + epsilon)
    scaled = (wide * gain_ref[...]).astype(jnp.bfloat16)
    product = jnp.dot(scaled, both_ref[...], preferred_element_type=jnp.float32)
    product = (product * inverse).astype(jnp.bfloat16)
    turned = jnp.dot(order_ref[...], product, preferred_element_type=jnp.float32)
    turned = turned.reshape(span, passages, chunks * LANES).astype(jnp.bfloat16)
    for chunk in range(chunks):
        start = pl.multiple_of(chunk * body + share * passages, TILE)
        out_ref[:, pl.ds(start, passages), :] = turned[
            :, :, chunk * LANES : (chunk + 1) * LANES
        ]


def spread_store(ids, store, gain, key_weight, value_weight, holders):
    passages, length, width = store.shape
    head_width = key_weight.shape[1]
    rows = passages * SHARE_ROWS
    per_holder = passages * length // holders * (2 * head_width // LANES) + TILE
    groups = holders // SHARE_ROWS
    return pl.pallas_call(
        spread_kernel,
        grid=(groups, length // holders),
        in_specs=[
            pl.BlockSpec(ids.shape, lambda g, i: (0, 0)),
            pl.BlockSpec((passages, SHARE_ROWS, width), lambda g, i: (0, i * groups + g, 0)),
            pl.BlockSpec((1, width), lambda g, i: (0, 0)),
            pl.BlockSpec((width, head_width), lambda g, i: (0, 0)),
            pl.BlockSpec((width, head_width), lambda g, i: (0, 0)),
        ],
        out_specs=pl.BlockSpec((SHARE_ROWS, per_holder, LANES), lambda g, i: (g, 0, 0)),
        out_shape=jax.ShapeDtypeStruct((holders, per_holder, LANES), jnp.bfloat16),
        scratch_shapes=[
            pltpu.VMEM((rows, rows), jnp.bfloat16),
            pltpu.VMEM((width, 2 * head_width), jnp.bfloat16),
        ],
        name="spread_store",
    )(ids, store, gain.reshape(1, width), key_weight, value_weight)


def select_kernel(blocks, shares, held_ref, out_ref, table_ref):
    step = pl.program_id(0)
    owners, length, _ = held_ref.shape
    passages = table_ref.shape[0] // owners
    width = table_ref.shape[1]
    chunks = width // shares // LANES

    @pl.when(step == 0)
    def _():
        for owner in range(owners):
            rows = slice(owner * passages, (owner + 1) * passages)
            for share in range(shares):
                for chunk in range(chunks):
                    source = (chunk * shares + share) * passages
                    lane = (share * chunks + chunk) * LANES
                    table_ref[rows, lane : lane + LANES] = held_ref[
                        owner, source : source + passages, :
                    ]

    spot = lax.broadcasted_iota(jnp.int32, (TILE, table_ref.shape[0]), 1).astype(jnp.float32)
    early = lax.broadcasted_iota(jnp.int32, (TILE, 1), 0) < NPB
    chosen = []
    for reader in range(SELECT_READERS):
        tile = held_ref[step * SELECT_READERS + reader, length - TILE :, :].astype(jnp.float32)
        wanted = tile[:, :blocks] * float(passages) + tile[:, blocks : 2 * blocks]
        for pair in range(0, blocks, 2):
            mine = jnp.where(early, wanted[:, pair : pair + 1], wanted[:, pair + 1 : pair + 2])
            chosen.append(jnp.where(spot == mine, 1.0, 0.0))
    chosen = jnp.concatenate(chosen, axis=0).astype(jnp.bfloat16)
    out_ref[...] = jnp.dot(chosen, table_ref[...], preferred_element_type=jnp.float32).astype(
        jnp.bfloat16
    )


def select_rows(held, blocks, passages, shares, width):
    owners = held.shape[0]
    step_rows = SELECT_READERS * blocks * NPB
    return pl.pallas_call(
        lambda *refs: select_kernel(blocks, shares, *refs),
        grid=(owners // SELECT_READERS,),
        in_specs=[whole],
        out_specs=pl.BlockSpec((step_rows, shares * width), lambda i: (i, 0)),
        out_shape=jax.ShapeDtypeStruct((owners * blocks * NPB, shares * width), jnp.bfloat16),
        scratch_shapes=[pltpu.VMEM((owners * passages, shares * width), jnp.bfloat16)],
        name="select_rows",
    )(held)


def attend_kernel(query_ref, gate_ref, table_ref, out_ref, keys_ref, scores_ref):
    holders, slots, _ = table_ref.shape
    rows, width = query_ref.shape
    both = 2 * width
    heads = width // HD
    early = lax.broadcasted_iota(jnp.int32, (holders, TILE, both), 1) < NPB
    for pair in range(slots // TILE):
        here = slice(pair * TILE, (pair + 1) * TILE)
        first = table_ref[:, here, :both].astype(jnp.float32)
        second = table_ref[:, here, both:].astype(jnp.float32)
        tables = (
            jnp.where(early, first, pltpu.roll(second, NPB, 1)),
            jnp.where(early, pltpu.roll(first, NPB, 1), second),
        )
        for place, table in enumerate(tables):
            keys_ref[2 * pair + place] = table.reshape(holders * TILE, both).astype(jnp.bfloat16)
    for head in range(heads):
        cols = slice(head * HD, (head + 1) * HD)
        for block in range(rows // BLK):
            mine = slice(block * BLK, (block + 1) * BLK)
            scores_ref[head, mine, :] = lax.dot_general(
                query_ref[mine, cols],
                keys_ref[block, :, cols],
                (((1,), (1,)), ((), ())),
                preferred_element_type=jnp.float32,
            ) * HD ** (-0.5)
    for head in range(heads):
        cols = slice(head * HD, (head + 1) * HD)
        late = slice(width + head * HD, width + (head + 1) * HD)
        scores = scores_ref[head]
        weights = jnp.exp(scores - jnp.max(scores, axis=-1, keepdims=True))
        total = jnp.sum(weights, axis=-1, keepdims=True)
        probabilities = (weights * (1.0 / total)).astype(jnp.bfloat16)
        for block in range(rows // BLK):
            mine = slice(block * BLK, (block + 1) * BLK)
            attended = jnp.dot(
                probabilities[mine, :], keys_ref[block, :, late], preferred_element_type=jnp.float32
            )
            out_ref[mine, cols] = (attended * gate_ref[mine, head : head + 1]).astype(jnp.bfloat16)


def attend(queries, gates, table, half):
    rows, width = queries.shape
    rows = rows // 2
    holders, slots, both = table.shape
    return pl.pallas_call(
        attend_kernel,
        grid=(1,),
        in_specs=[
            pl.BlockSpec((rows, width), lambda i: (half, 0)),
            pl.BlockSpec((rows, gates.shape[1]), lambda i: (half, 0)),
            pl.BlockSpec((holders, slots // 2, both), lambda i: (0, half, 0)),
        ],
        out_specs=pl.BlockSpec((rows, width), lambda i: (0, 0)),
        out_shape=jax.ShapeDtypeStruct((rows, width), jnp.bfloat16),
        scratch_shapes=[
            pltpu.VMEM((rows // BLK, holders * TILE, both // 2), jnp.bfloat16),
            pltpu.VMEM((width // HD, rows, holders * TILE), jnp.float32),
        ],
        name="attend",
    )(queries, gates, table)


def per_device(
    tokens,
    norm_gain,
    pool_weight,
    pool_scale,
    query_weight,
    gate_weight,
    key_weight,
    value_weight,
    out_weight,
    passage_gain,
    passage_store,
    passage_ids,
):
    head_index = lax.axis_index("tp")
    tp_count = lax.axis_size("tp")
    tok_rows, width_local = tokens.shape
    full_width = width_local * tp_count
    local_heads = query_weight.shape[1] // HD
    st_count = lax.axis_size("st")
    passages = passage_store.shape[0]
    shares = PLEN // st_count
    spread = spread_store(
        passage_ids.T, passage_store, passage_gain, key_weight, value_weight, st_count
    )
    held = lax.all_to_all(spread, "st", split_axis=0, concat_axis=0, tiled=True)
    width_both = key_weight.shape[1] + value_weight.shape[1]
    packed = select_rows(held, tok_rows // BLK, passages, shares, width_both)
    returned = lax.all_to_all(
        packed.reshape(st_count, -1, shares * width_both),
        "st",
        split_axis=0,
        concat_axis=0,
        tiled=True,
    )

    wide_tokens = tokens.astype(jnp.float32)
    square_sums = lax.psum(jnp.sum(wide_tokens * wide_tokens, axis=1), "tp")
    inverse = lax.rsqrt(square_sums / full_width + epsilon)
    gain_local = lax.dynamic_slice_in_dim(norm_gain, head_index * width_local, width_local)
    normed = (wide_tokens * inverse[:, None] * gain_local[None, :]).astype(jnp.bfloat16)
    up = [(i, (i + 1) % tp_count) for i in range(tp_count)]
    down = [(i, (i - 1) % tp_count) for i in range(tp_count)]
    across = [(i, (i + 2) % tp_count) for i in range(tp_count)]
    half = tok_rows // 2
    turned = (head_index + jnp.array([0, tp_count - 1, 1, 2], dtype=jnp.int32)) % tp_count
    before = lax.ppermute(normed, "tp", up)
    after = lax.ppermute(normed, "tp", down)
    far = lax.ppermute(normed, "tp", across)
    columns = jnp.concatenate([normed, before, after, far], axis=1)

    sequences = tok_rows // SEQ_LEN
    window = jnp.left_shift(jnp.int32(2), head_index)
    grouped = normed.astype(jnp.float32).reshape(sequences, SEQ_LEN, width_local)
    total = grouped
    for level in range(GROUPS):
        shift = 2**level
        moved = jnp.pad(total, ((0, 0), (shift, 0), (0, 0)))[:, :SEQ_LEN]
        total = jnp.where(level <= head_index, total + moved, total)
    position = jnp.arange(SEQ_LEN, dtype=jnp.int32)
    divisor = jnp.minimum(position + 1, window).astype(jnp.float32)
    pooled = (
        (total / divisor[None, :, None] - grouped)
        .astype(jnp.bfloat16)
        .reshape(tok_rows, width_local)
    )
    base = (
        jnp.dot(pooled, pool_weight[0], preferred_element_type=jnp.float32) * pool_scale[None, :]
    )

    def turn(weight):
        pieces = weight.reshape(tp_count, weight.shape[0] // tp_count, weight.shape[1])
        return jnp.take(pieces, turned, axis=0, mode="clip")

    gate_columns = lax.dynamic_slice_in_dim(
        gate_weight, head_index * local_heads, local_heads, axis=1
    )
    query_sum = jnp.dot(
        columns, turn(query_weight).reshape(query_weight.shape), preferred_element_type=jnp.float32
    )
    gate_sum = jnp.dot(
        columns, turn(gate_columns).reshape(gate_columns.shape), preferred_element_type=jnp.float32
    )
    queries = query_sum.astype(jnp.bfloat16)
    gating = jax.nn.sigmoid(gate_sum)

    weights = turn(out_weight)
    near = weights[:3].reshape(-1, width_local)
    queries, gating, base, near, distant = lax.optimization_barrier(
        (queries, gating, base, near, weights[3])
    )

    low = attend(queries, gating, returned, 0)
    low_before = lax.ppermute(low, "tp", up)
    low_after = lax.ppermute(low, "tp", down)
    high = attend(queries, gating, returned, 1)
    high_before = lax.ppermute(high, "tp", up)
    high_after = lax.ppermute(high, "tp", down)
    low_far = lax.ppermute(low_before, "tp", up)
    high_far = lax.ppermute(high_after, "tp", down)
    low_near = jnp.concatenate([low, low_before, low_after], axis=1)
    low_base = base[:half] + jnp.dot(low_near, near, preferred_element_type=jnp.float32)
    high_near = jnp.concatenate([high, high_before, high_after], axis=1)
    high_base = base[half:] + jnp.dot(high_near, near, preferred_element_type=jnp.float32)
    low_base, high_base = lax.optimization_barrier((low_base, high_base))
    far = jnp.concatenate([low_far, high_far], axis=0)
    base = jnp.concatenate([low_base, high_base], axis=0)
    return (base + jnp.dot(far, distant, preferred_element_type=jnp.float32)).astype(jnp.bfloat16)


def solution(mesh):
    in_specs = (
        P(("grp", "st"), "tp"),
        P(),
        P("tp", None, None),
        P("tp"),
        P(None, "tp"),
        P(),
        P(None, "tp"),
        P(None, "tp"),
        P(None, "tp"),
        P(),
        P(("grp", "st"), None, None),
        P(("grp", "st"), None),
    )
    out_specs = P(("grp", "st"), "tp")
    return jax.shard_map(per_device, mesh=mesh, in_specs=in_specs, out_specs=out_specs, check_vma=False)
```

```python
import jax
import jax.numpy as jnp
from jax import lax
from jax.experimental import pallas as pl
from jax.experimental.pallas import tpu as pltpu
from jax.sharding import PartitionSpec as P

HD = 128
GROUPS = 4
SEQ_LEN = 256
BLK = 128
NPB = 4
PLEN = 64

epsilon = 1e-06
LANES = 128
TILE = 8
SHARE_ROWS = 16
SELECT_READERS = 16
whole = pl.BlockSpec(memory_space=pltpu.VMEM)


def spread_kernel(ids_ref, store_ref, gain_ref, key_ref, value_ref, out_ref, turn_ref, both_ref):
    group, share = pl.program_id(0), pl.program_id(1)
    passages, span, width = store_ref.shape
    rows = passages * span
    length = out_ref.shape[1]
    half = key_ref.shape[1]
    chunks = 2 * half // LANES
    body = (length - TILE) // chunks

    @pl.when((group == 0) & (share == 0))
    def _():
        both_ref[:, :half] = key_ref[...]
        both_ref[:, half:] = value_ref[...]

    @pl.when(share == 0)
    def _():
        ids = ids_ref[...]
        ids = jnp.concatenate([ids] * (TILE // NPB), axis=0)
        owner = lax.div(ids, jnp.int32(passages))
        inside = ids - owner * passages
        spare = jnp.zeros((TILE, LANES - 2 * ids.shape[1]), jnp.int32)
        tile = jnp.concatenate([owner, inside, spare], axis=1)
        tile = tile.astype(jnp.float32).astype(jnp.bfloat16)
        out_ref[:, length - TILE :, :] = jnp.broadcast_to(tile, (span, TILE, LANES))

    wide = store_ref[...].astype(jnp.float32).reshape(rows, width)
    inverse = lax.rsqrt(jnp.mean(wide * wide, axis=-1, keepdims=True) + epsilon)
    scaled = (wide * gain_ref[...]).astype(jnp.bfloat16)
    product = jnp.dot(scaled, both_ref[...], preferred_element_type=jnp.float32)
    product = product * inverse
    for chunk in range(chunks):
        turn_ref[chunk] = product[:, chunk * LANES : (chunk + 1) * LANES]
    for chunk in range(chunks):
        start = pl.multiple_of(chunk * body + share * passages, TILE)
        for holder in range(span):
            turned = turn_ref[chunk, pl.ds(holder, passages, stride=span), :]
            out_ref[holder, pl.ds(start, passages), :] = turned.astype(jnp.bfloat16)


def spread_store(ids, store, gain, key_weight, value_weight, holders):
    passages, length, width = store.shape
    head_width = key_weight.shape[1]
    rows = passages * SHARE_ROWS
    per_holder = passages * length // holders * (2 * head_width // LANES) + TILE
    groups = holders // SHARE_ROWS
    return pl.pallas_call(
        spread_kernel,
        grid=(groups, length // holders),
        in_specs=[
            pl.BlockSpec(ids.shape, lambda g, i: (0, 0)),
            pl.BlockSpec((passages, SHARE_ROWS, width), lambda g, i: (0, i * groups + g, 0)),
            pl.BlockSpec((1, width), lambda g, i: (0, 0)),
            pl.BlockSpec((width, head_width), lambda g, i: (0, 0)),
            pl.BlockSpec((width, head_width), lambda g, i: (0, 0)),
        ],
        out_specs=pl.BlockSpec((SHARE_ROWS, per_holder, LANES), lambda g, i: (g, 0, 0)),
        out_shape=jax.ShapeDtypeStruct((holders, per_holder, LANES), jnp.bfloat16),
        scratch_shapes=[
            pltpu.VMEM((2 * head_width // LANES, rows, LANES), jnp.float32),
            pltpu.VMEM((width, 2 * head_width), jnp.bfloat16),
        ],
        name="spread_store",
    )(ids, store, gain.reshape(1, width), key_weight, value_weight)


def select_kernel(blocks, shares, held_ref, out_ref, table_ref):
    step = pl.program_id(0)
    owners, length, _ = held_ref.shape
    passages = table_ref.shape[0] // owners
    width = table_ref.shape[1]
    chunks = width // shares // LANES

    @pl.when(step == 0)
    def _():
        for owner in range(owners):
            rows = slice(owner * passages, (owner + 1) * passages)
            for share in range(shares):
                for chunk in range(chunks):
                    source = (chunk * shares + share) * passages
                    lane = (share * chunks + chunk) * LANES
                    table_ref[rows, lane : lane + LANES] = held_ref[
                        owner, source : source + passages, :
                    ]

    spot = lax.broadcasted_iota(jnp.int32, (TILE, table_ref.shape[0]), 1).astype(jnp.float32)
    early = lax.broadcasted_iota(jnp.int32, (TILE, 1), 0) < NPB
    chosen = []
    for reader in range(SELECT_READERS):
        tile = held_ref[step * SELECT_READERS + reader, length - TILE :, :].astype(jnp.float32)
        wanted = tile[:, :blocks] * float(passages) + tile[:, blocks : 2 * blocks]
        for pair in range(0, blocks, 2):
            mine = jnp.where(early, wanted[:, pair : pair + 1], wanted[:, pair + 1 : pair + 2])
            chosen.append(jnp.where(spot == mine, 1.0, 0.0))
    chosen = jnp.concatenate(chosen, axis=0).astype(jnp.bfloat16)
    out_ref[...] = jnp.dot(chosen, table_ref[...], preferred_element_type=jnp.float32).astype(
        jnp.bfloat16
    )


def select_rows(held, blocks, passages, shares, width):
    owners = held.shape[0]
    step_rows = SELECT_READERS * blocks * NPB
    return pl.pallas_call(
        lambda *refs: select_kernel(blocks, shares, *refs),
        grid=(owners // SELECT_READERS,),
        in_specs=[whole],
        out_specs=pl.BlockSpec((step_rows, shares * width), lambda i: (i, 0)),
        out_shape=jax.ShapeDtypeStruct((owners * blocks * NPB, shares * width), jnp.bfloat16),
        scratch_shapes=[pltpu.VMEM((owners * passages, shares * width), jnp.bfloat16)],
        name="select_rows",
    )(held)


def attend_kernel(query_ref, gate_ref, table_ref, out_ref, keys_ref, scores_ref):
    holders, slots, _ = table_ref.shape
    rows, width = query_ref.shape
    both = 2 * width
    heads = width // HD
    early = lax.broadcasted_iota(jnp.int32, (holders, TILE, both), 1) < NPB
    for pair in range(slots // TILE):
        here = slice(pair * TILE, (pair + 1) * TILE)
        first = table_ref[:, here, :both].astype(jnp.float32)
        second = table_ref[:, here, both:].astype(jnp.float32)
        tables = (
            jnp.where(early, first, pltpu.roll(second, NPB, 1)),
            jnp.where(early, pltpu.roll(first, NPB, 1), second),
        )
        for place, table in enumerate(tables):
            keys_ref[2 * pair + place] = table.reshape(holders * TILE, both).astype(jnp.bfloat16)
    for head in range(heads):
        cols = slice(head * HD, (head + 1) * HD)
        for block in range(rows // BLK):
            mine = slice(block * BLK, (block + 1) * BLK)
            scores_ref[head, mine, :] = lax.dot_general(
                query_ref[mine, cols],
                keys_ref[block, :, cols],
                (((1,), (1,)), ((), ())),
                preferred_element_type=jnp.float32,
            ) * HD ** (-0.5)
    for head in range(heads):
        cols = slice(head * HD, (head + 1) * HD)
        late = slice(width + head * HD, width + (head + 1) * HD)
        scores = scores_ref[head]
        weights = jnp.exp(scores - jnp.max(scores, axis=-1, keepdims=True))
        total = jnp.sum(weights, axis=-1, keepdims=True)
        probabilities = (weights * (1.0 / total)).astype(jnp.bfloat16)
        for block in range(rows // BLK):
            mine = slice(block * BLK, (block + 1) * BLK)
            attended = jnp.dot(
                probabilities[mine, :], keys_ref[block, :, late], preferred_element_type=jnp.float32
            )
            out_ref[mine, cols] = (attended * gate_ref[mine, head : head + 1]).astype(jnp.bfloat16)


def attend(queries, gates, table, half):
    rows, width = queries.shape
    rows = rows // 2
    holders, slots, both = table.shape
    span = rows // BLK * NPB
    return pl.pallas_call(
        attend_kernel,
        grid=(1,),
        in_specs=[
            pl.BlockSpec((rows, width), lambda i: (half, 0)),
            pl.BlockSpec((rows, gates.shape[1]), lambda i: (half, 0)),
            pl.BlockSpec((holders, span, both), lambda i: (0, slots // span - 1, 0)),
        ],
        out_specs=pl.BlockSpec((rows, width), lambda i: (0, 0)),
        out_shape=jax.ShapeDtypeStruct((rows, width), jnp.bfloat16),
        scratch_shapes=[
            pltpu.VMEM((rows // BLK, holders * TILE, both // 2), jnp.bfloat16),
            pltpu.VMEM((width // HD, rows, holders * TILE), jnp.float32),
        ],
        name="attend",
    )(queries, gates, table)


def per_device(
    tokens,
    norm_gain,
    pool_weight,
    pool_scale,
    query_weight,
    gate_weight,
    key_weight,
    value_weight,
    out_weight,
    passage_gain,
    passage_store,
    passage_ids,
):
    head_index = lax.axis_index("tp")
    tp_count = lax.axis_size("tp")
    tok_rows, width_local = tokens.shape
    full_width = width_local * tp_count
    local_heads = query_weight.shape[1] // HD
    st_count = lax.axis_size("st")
    passages = passage_store.shape[0]
    shares = PLEN // st_count
    spread = spread_store(
        passage_ids.T, passage_store, passage_gain, key_weight, value_weight, st_count
    )
    held = lax.all_to_all(spread, "st", split_axis=0, concat_axis=0, tiled=True)
    width_both = key_weight.shape[1] + value_weight.shape[1]
    packed = select_rows(held, tok_rows // BLK, passages, shares, width_both)
    returned = lax.all_to_all(
        packed.reshape(st_count, -1, shares * width_both),
        "st",
        split_axis=0,
        concat_axis=0,
        tiled=True,
    )

    wide_tokens = tokens.astype(jnp.float32)
    square_sums = lax.psum(jnp.sum(wide_tokens * wide_tokens, axis=1), "tp")
    inverse = lax.rsqrt(square_sums / full_width + epsilon)
    gain_local = lax.dynamic_slice_in_dim(norm_gain, head_index * width_local, width_local)
    normed = (wide_tokens * inverse[:, None] * gain_local[None, :]).astype(jnp.bfloat16)
    up = [(i, (i + 1) % tp_count) for i in range(tp_count)]
    down = [(i, (i - 1) % tp_count) for i in range(tp_count)]
    across = [(i, (i + 2) % tp_count) for i in range(tp_count)]
    half = tok_rows // 2
    turned = (head_index + jnp.array([0, tp_count - 1, 1, 2], dtype=jnp.int32)) % tp_count
    before = lax.ppermute(normed, "tp", up)
    after = lax.ppermute(normed, "tp", down)
    far = lax.ppermute(normed, "tp", across)
    columns = jnp.concatenate([normed, before, after, far], axis=1)

    sequences = tok_rows // SEQ_LEN
    window = jnp.left_shift(jnp.int32(2), head_index)
    grouped = normed.astype(jnp.float32).reshape(sequences, SEQ_LEN, width_local)
    total = grouped
    for level in range(GROUPS):
        shift = 2**level
        moved = jnp.pad(total, ((0, 0), (shift, 0), (0, 0)))[:, :SEQ_LEN]
        total = jnp.where(level <= head_index, total + moved, total)
    position = jnp.arange(SEQ_LEN, dtype=jnp.int32)
    divisor = jnp.minimum(position + 1, window).astype(jnp.float32)
    pooled = (
        (total / divisor[None, :, None] - grouped)
        .astype(jnp.bfloat16)
        .reshape(tok_rows, width_local)
    )
    base = (
        jnp.dot(pooled, pool_weight[0], preferred_element_type=jnp.float32) * pool_scale[None, :]
    )

    def turn(weight):
        pieces = weight.reshape(tp_count, weight.shape[0] // tp_count, weight.shape[1])
        return jnp.take(pieces, turned, axis=0, mode="clip")

    gate_columns = lax.dynamic_slice_in_dim(
        gate_weight, head_index * local_heads, local_heads, axis=1
    )
    query_sum = jnp.dot(
        columns, turn(query_weight).reshape(query_weight.shape), preferred_element_type=jnp.float32
    )
    gate_sum = jnp.dot(
        columns, turn(gate_columns).reshape(gate_columns.shape), preferred_element_type=jnp.float32
    )
    queries = query_sum.astype(jnp.bfloat16)
    gating = jax.nn.sigmoid(gate_sum)

    weights = turn(out_weight)
    near = weights[:3].reshape(-1, width_local)
    queries, gating, base, near, distant = lax.optimization_barrier(
        (queries, gating, base, near, weights[3])
    )

    low = attend(queries, gating, returned[:, : returned.shape[1] // 2], 0)
    low_before = lax.ppermute(low, "tp", up)
    low_after = lax.ppermute(low, "tp", down)
    high = attend(queries, gating, returned, 1)
    high_before = lax.ppermute(high, "tp", up)
    high_after = lax.ppermute(high, "tp", down)
    low_far = lax.ppermute(low_before, "tp", up)
    high_far = lax.ppermute(high_after, "tp", down)
    low_near = jnp.concatenate([low, low_before, low_after], axis=1)
    low_base = base[:half] + jnp.dot(low_near, near, preferred_element_type=jnp.float32)
    high_near = jnp.concatenate([high, high_before, high_after], axis=1)
    high_base = base[half:] + jnp.dot(high_near, near, preferred_element_type=jnp.float32)
    low_base, high_base = lax.optimization_barrier((low_base, high_base))
    far = jnp.concatenate([low_far, high_far], axis=0)
    base = jnp.concatenate([low_base, high_base], axis=0)
    return (base + jnp.dot(far, distant, preferred_element_type=jnp.float32)).astype(jnp.bfloat16)


def solution(mesh):
    in_specs = (
        P(("grp", "st"), "tp"),
        P(),
        P("tp", None, None),
        P("tp"),
        P(None, "tp"),
        P(),
        P(None, "tp"),
        P(None, "tp"),
        P(None, "tp"),
        P(),
        P(("grp", "st"), None, None),
        P(("grp", "st"), None),
    )
    out_specs = P(("grp", "st"), "tp")
    return jax.shard_map(per_device, mesh=mesh, in_specs=in_specs, out_specs=out_specs, check_vma=False)
```

```python
import jax
import jax.numpy as jnp
from jax import lax
from jax.experimental import pallas as pl
from jax.experimental.pallas import tpu as pltpu
from jax.sharding import PartitionSpec as P

HD = 128
GROUPS = 4
SEQ_LEN = 256
BLK = 128
NPB = 4
PLEN = 64

epsilon = 1e-06
LANES = 128
TILE = 8
SHARE_ROWS = 16
SELECT_READERS = 16
whole = pl.BlockSpec(memory_space=pltpu.VMEM)


def spread_kernel(ids_ref, store_ref, gain_ref, key_ref, value_ref, out_ref, turn_ref, both_ref):
    group, share = pl.program_id(0), pl.program_id(1)
    passages, span, width = store_ref.shape
    rows = passages * span
    length = out_ref.shape[1]
    half = key_ref.shape[1]
    chunks = 2 * half // LANES
    body = (length - TILE) // chunks

    @pl.when((group == 0) & (share == 0))
    def _():
        both_ref[:, :half] = key_ref[...]
        both_ref[:, half:] = value_ref[...]

    @pl.when(share == 0)
    def _():
        ids = ids_ref[...]
        ids = jnp.concatenate([ids] * (TILE // NPB), axis=0)
        owner = lax.div(ids, jnp.int32(passages))
        inside = ids - owner * passages
        spare = jnp.zeros((TILE, LANES - 2 * ids.shape[1]), jnp.int32)
        tile = jnp.concatenate([owner, inside, spare], axis=1)
        tile = tile.astype(jnp.float32).astype(jnp.bfloat16)
        out_ref[:, length - TILE :, :] = jnp.broadcast_to(tile, (span, TILE, LANES))

    wide = store_ref[...].astype(jnp.float32).reshape(rows, width)
    inverse = lax.rsqrt(jnp.mean(wide * wide, axis=-1, keepdims=True) + epsilon)
    scaled = (wide * gain_ref[...]).astype(jnp.bfloat16)
    product = jnp.dot(scaled, both_ref[...], preferred_element_type=jnp.float32)
    product = product * inverse
    for chunk in range(chunks):
        turn_ref[chunk] = product[:, chunk * LANES : (chunk + 1) * LANES]
    for chunk in range(chunks):
        start = pl.multiple_of(chunk * body + share * passages, TILE)
        for holder in range(span):
            turned = turn_ref[chunk, pl.ds(holder, passages, stride=span), :]
            out_ref[holder, pl.ds(start, passages), :] = turned.astype(jnp.bfloat16)


def spread_store(ids, store, gain, key_weight, value_weight, holders):
    passages, length, width = store.shape
    head_width = key_weight.shape[1]
    rows = passages * SHARE_ROWS
    per_holder = passages * length // holders * (2 * head_width // LANES) + TILE
    groups = holders // SHARE_ROWS
    return pl.pallas_call(
        spread_kernel,
        grid=(groups, length // holders),
        in_specs=[
            pl.BlockSpec(ids.shape, lambda g, i: (0, 0)),
            pl.BlockSpec((passages, SHARE_ROWS, width), lambda g, i: (0, i * groups + g, 0)),
            pl.BlockSpec((1, width), lambda g, i: (0, 0)),
            pl.BlockSpec((width, head_width), lambda g, i: (0, 0)),
            pl.BlockSpec((width, head_width), lambda g, i: (0, 0)),
        ],
        out_specs=pl.BlockSpec((SHARE_ROWS, per_holder, LANES), lambda g, i: (g, 0, 0)),
        out_shape=jax.ShapeDtypeStruct((holders, per_holder, LANES), jnp.bfloat16),
        scratch_shapes=[
            pltpu.VMEM((2 * head_width // LANES, rows, LANES), jnp.float32),
            pltpu.VMEM((width, 2 * head_width), jnp.bfloat16),
        ],
        name="spread_store",
    )(ids, store, gain.reshape(1, width), key_weight, value_weight)


def select_kernel(blocks, shares, held_ref, out_ref, table_ref):
    step = pl.program_id(0)
    owners, length, _ = held_ref.shape
    passages = table_ref.shape[0] // owners
    width = table_ref.shape[1]
    chunks = width // shares // LANES

    @pl.when(step == 0)
    def _():
        for owner in range(owners):
            rows = slice(owner * passages, (owner + 1) * passages)
            for share in range(shares):
                for chunk in range(chunks):
                    source = (chunk * shares + share) * passages
                    lane = (share * chunks + chunk) * LANES
                    table_ref[rows, lane : lane + LANES] = held_ref[
                        owner, source : source + passages, :
                    ]

    spot = lax.broadcasted_iota(jnp.int32, (TILE, table_ref.shape[0]), 1).astype(jnp.float32)
    early = lax.broadcasted_iota(jnp.int32, (TILE, 1), 0) < NPB
    chosen = []
    for reader in range(SELECT_READERS):
        tile = held_ref[step * SELECT_READERS + reader, length - TILE :, :].astype(jnp.float32)
        wanted = tile[:, :blocks] * float(passages) + tile[:, blocks : 2 * blocks]
        for pair in range(0, blocks, 2):
            mine = jnp.where(early, wanted[:, pair : pair + 1], wanted[:, pair + 1 : pair + 2])
            chosen.append(jnp.where(spot == mine, 1.0, 0.0))
    chosen = jnp.concatenate(chosen, axis=0).astype(jnp.bfloat16)
    out_ref[...] = jnp.dot(chosen, table_ref[...], preferred_element_type=jnp.float32).astype(
        jnp.bfloat16
    )


def select_rows(held, blocks, passages, shares, width):
    owners = held.shape[0]
    step_rows = SELECT_READERS * blocks * NPB
    return pl.pallas_call(
        lambda *refs: select_kernel(blocks, shares, *refs),
        grid=(owners // SELECT_READERS,),
        in_specs=[whole],
        out_specs=pl.BlockSpec((step_rows, shares * width), lambda i: (i, 0)),
        out_shape=jax.ShapeDtypeStruct((owners * blocks * NPB, shares * width), jnp.bfloat16),
        scratch_shapes=[pltpu.VMEM((owners * passages, shares * width), jnp.bfloat16)],
        name="select_rows",
    )(held)


def attend_kernel(query_ref, gate_ref, table_ref, out_ref, keys_ref, scores_ref):
    holders, slots, _ = table_ref.shape
    rows, width = query_ref.shape
    both = 2 * width
    heads = width // HD
    early = lax.broadcasted_iota(jnp.int32, (holders, TILE, both), 1) < NPB
    for pair in range(slots // TILE):
        here = slice(pair * TILE, (pair + 1) * TILE)
        first = table_ref[:, here, :both].astype(jnp.float32)
        second = table_ref[:, here, both:].astype(jnp.float32)
        tables = (
            jnp.where(early, first, pltpu.roll(second, NPB, 1)),
            jnp.where(early, pltpu.roll(first, NPB, 1), second),
        )
        for place, table in enumerate(tables):
            keys_ref[2 * pair + place] = table.reshape(holders * TILE, both).astype(jnp.bfloat16)
    for head in range(heads):
        cols = slice(head * HD, (head + 1) * HD)
        for block in range(rows // BLK):
            mine = slice(block * BLK, (block + 1) * BLK)
            scores_ref[head, mine, :] = lax.dot_general(
                query_ref[mine, cols],
                keys_ref[block, :, cols],
                (((1,), (1,)), ((), ())),
                preferred_element_type=jnp.float32,
            ) * HD ** (-0.5)
    for head in range(heads):
        cols = slice(head * HD, (head + 1) * HD)
        late = slice(width + head * HD, width + (head + 1) * HD)
        scores = scores_ref[head]
        weights = jnp.exp(scores - jnp.max(scores, axis=-1, keepdims=True))
        total = jnp.sum(weights, axis=-1, keepdims=True)
        probabilities = (weights * (1.0 / total)).astype(jnp.bfloat16)
        for block in range(rows // BLK):
            mine = slice(block * BLK, (block + 1) * BLK)
            attended = jnp.dot(
                probabilities[mine, :], keys_ref[block, :, late], preferred_element_type=jnp.float32
            )
            out_ref[mine, cols] = (attended * gate_ref[mine, head : head + 1]).astype(jnp.bfloat16)


def attend(queries, gates, table, half):
    rows, width = queries.shape
    rows = rows // 2
    holders, slots, both = table.shape
    return pl.pallas_call(
        attend_kernel,
        grid=(1,),
        in_specs=[
            pl.BlockSpec((rows, width), lambda i: (half, 0)),
            pl.BlockSpec((rows, gates.shape[1]), lambda i: (half, 0)),
            pl.BlockSpec((holders, slots // 2, both), lambda i: (0, half, 0)),
        ],
        out_specs=pl.BlockSpec((rows, width), lambda i: (0, 0)),
        out_shape=jax.ShapeDtypeStruct((rows, width), jnp.bfloat16),
        scratch_shapes=[
            pltpu.VMEM((rows // BLK, holders * TILE, both // 2), jnp.bfloat16),
            pltpu.VMEM((width // HD, rows, holders * TILE), jnp.float32),
        ],
        name="attend",
    )(queries, gates, table)


def per_device(
    tokens,
    norm_gain,
    pool_weight,
    pool_scale,
    query_weight,
    gate_weight,
    key_weight,
    value_weight,
    out_weight,
    passage_gain,
    passage_store,
    passage_ids,
):
    head_index = lax.axis_index("tp")
    tp_count = lax.axis_size("tp")
    tok_rows, width_local = tokens.shape
    full_width = width_local * tp_count
    local_heads = query_weight.shape[1] // HD
    st_count = lax.axis_size("st")
    passages = passage_store.shape[0]
    shares = PLEN // st_count
    spread = spread_store(
        passage_ids.T, passage_store, passage_gain, key_weight, value_weight, st_count
    )
    held = lax.all_to_all(spread, "st", split_axis=0, concat_axis=0, tiled=True)
    width_both = key_weight.shape[1] + value_weight.shape[1]
    packed = select_rows(held, tok_rows // BLK, passages, shares, width_both)
    returned = lax.all_to_all(
        packed.reshape(st_count, -1, shares * width_both),
        "st",
        split_axis=0,
        concat_axis=0,
        tiled=True,
    )

    wide_tokens = tokens.astype(jnp.float32)
    square_sums = lax.psum(jnp.sum(wide_tokens * wide_tokens, axis=1), "tp")
    inverse = lax.rsqrt(square_sums / full_width + epsilon)
    gain_local = lax.dynamic_slice_in_dim(norm_gain, head_index * width_local, width_local)
    normed = (wide_tokens * inverse[:, None] * gain_local[None, :]).astype(jnp.bfloat16)
    up = [(i, (i + 1) % tp_count) for i in range(tp_count)]
    down = [(i, (i - 1) % tp_count) for i in range(tp_count)]
    across = [(i, (i + 2) % tp_count) for i in range(tp_count)]
    half = tok_rows // 2
    turned = (head_index + jnp.array([0, tp_count - 1, 1, 2], dtype=jnp.int32)) % tp_count
    before = lax.ppermute(normed, "tp", up)
    after = lax.ppermute(normed, "tp", down)
    far = lax.ppermute(normed, "tp", across)
    columns = jnp.concatenate([normed, before, after, far], axis=1)

    sequences = tok_rows // SEQ_LEN
    window = jnp.left_shift(jnp.int32(2), head_index)
    grouped = normed.astype(jnp.float32).reshape(sequences, SEQ_LEN, width_local)
    total = grouped
    for level in range(GROUPS):
        shift = 2**level
        moved = jnp.pad(total, ((0, 0), (shift, 0), (0, 0)))[:, :SEQ_LEN]
        total = jnp.where(level <= head_index, total + moved, total)
    position = jnp.arange(SEQ_LEN, dtype=jnp.int32)
    divisor = jnp.minimum(position + 1, window).astype(jnp.float32)
    pooled = (
        (total / divisor[None, :, None] - grouped)
        .astype(jnp.bfloat16)
        .reshape(tok_rows, width_local)
    )
    base = (
        jnp.dot(pooled, pool_weight[0], preferred_element_type=jnp.float32) * pool_scale[None, :]
    )

    def turn(weight):
        pieces = weight.reshape(tp_count, weight.shape[0] // tp_count, weight.shape[1])
        return jnp.take(pieces, turned, axis=0, mode="clip")

    gate_columns = lax.dynamic_slice_in_dim(
        gate_weight, head_index * local_heads, local_heads, axis=1
    )
    query_sum = jnp.dot(
        columns, turn(query_weight).reshape(query_weight.shape), preferred_element_type=jnp.float32
    )
    gate_sum = jnp.dot(
        columns, turn(gate_columns).reshape(gate_columns.shape), preferred_element_type=jnp.float32
    )
    queries = query_sum.astype(jnp.bfloat16)
    gating = jax.nn.sigmoid(gate_sum)

    weights = turn(out_weight)
    near = weights[:3].reshape(-1, width_local)
    queries, gating, base, near, distant = lax.optimization_barrier(
        (queries, gating, base, near, weights[3])
    )

    low = attend(queries, gating, returned, 0)
    low_before = lax.ppermute(low, "tp", up)
    low_after = lax.ppermute(low, "tp", down)
    high = attend(queries, gating, returned, 1)
    high_before = lax.ppermute(high, "tp", up)
    high_after = lax.ppermute(high, "tp", down)
    low_far = lax.ppermute(low_before, "tp", up)
    high_far = lax.ppermute(high_after, "tp", down)
    low_near = jnp.concatenate([low, low_before, low_after], axis=1)
    low_base = base[:half] + jnp.dot(low_near, near, preferred_element_type=jnp.float32)
    high_near = jnp.concatenate([high, high_before, high_after], axis=1)
    high_base = base[half:] + jnp.dot(high_near, near, preferred_element_type=jnp.float32)
    low_base, high_base = lax.optimization_barrier((low_base, high_base))
    far = jnp.concatenate([low_far, high_far], axis=0)
    base = jnp.concatenate([low_base, high_base], axis=0)
    return (base + jnp.dot(far, distant, preferred_element_type=jnp.float32)).astype(jnp.bfloat16)


def solution(mesh):
    in_specs = (
        P(("grp", "st"), "tp"),
        P(),
        P("tp", None, None),
        P("tp"),
        P(None, "tp"),
        P(),
        P(None, "tp"),
        P(None, "tp"),
        P(None, "tp"),
        P(),
        P(("grp", "st"), None, None),
        P(("grp", "st"), None),
    )
    out_specs = P(("grp", "st"), "tp")
    return jax.shard_map(per_device, mesh=mesh, in_specs=in_specs, out_specs=out_specs, check_vma=False)
```
